32 devices in a mesh: sp: 16 (over z, y, core), tp: 2 (over x).
Axes of the slice: x: 2, y: 2, z: 4, core: 2. Of those that a mesh axis runs over, the one named last changes fastest.
Arguments:
- query_rows: bfloat16 [10240, 1536], P('sp', 'tp'), may hold values from -8 to 8
- key_rows: bfloat16 [10240, 1536], P('sp', 'tp'), may hold values from -8 to 8
- value_rows: bfloat16 [10240, 1536], P('sp', 'tp'), may hold values from -6 to 6
- query_gain: bfloat16 [64], replicated, may hold values from 0.25 to 4.2
- key_gain: bfloat16 [64], replicated, may hold values from 0.25 to 4.2
- position_bias: bfloat16 [24, 320], P('tp'), may hold values from -165 to 3
- output_grad: bfloat16 [10240, 1536], P('sp', 'tp'), may hold values from -24 to 24
Outputs:
- query_grad: bfloat16 [10240, 1536], P('sp', 'tp')
- key_grad: bfloat16 [10240, 1536], P('sp', 'tp')
- value_grad: bfloat16 [10240, 1536], P('sp', 'tp')
- bias_grad: float32 [24, 320], P('tp')
- query_gain_grad: float32 [64], replicated
- key_gain_grad: float32 [64], replicated
The draws below stay inside these ranges and needn't reach their ends.
All inputs are finite; a program needn't handle non-finite values.
Results may differ from the reference program's by a relative error of at most 0.0055.
The reference program's roundings to bfloat16 on the way count: a program that leaves them out, or rounds other values in their place, can miss the bound.
Values may be sent and summed in bfloat16 or wider, within the bound.
A program may use at most 128 MiB of HBM per device.

```python
import jax
import jax.numpy as jnp
import numpy as np
from jax import lax

HEADS = 24
HEAD_DIM = 64
SEG = 64
LEFT = 8
CLIP = 256
TOK_DEV = 640
SEQ = 10240


def planted_pair(base):
    key_part = jax.random.normal(jax.random.fold_in(base, 101), (SEQ, HEADS * HEAD_DIM), jnp.float32)
    query_part = jax.random.normal(jax.random.fold_in(base, 202), (SEQ, HEADS * HEAD_DIM), jnp.float32)
    return (jnp.clip(query_part, -8.0, 8.0), jnp.clip(key_part, -8.0, 8.0))


def draw_query_rows(key, part):
    return planted_pair(key)[0].astype(jnp.bfloat16)


def draw_key_rows(key, part):
    return planted_pair(key)[1].astype(jnp.bfloat16)


def gain_of(base, salt):
    return 1.0 + 0.18 * jnp.clip(jax.random.normal(jax.random.fold_in(base, salt), (HEAD_DIM,), jnp.float32), -4.0, 4.0)


def draw_query_gain(key, part):
    return gain_of(key, 505).astype(jnp.bfloat16)


def draw_key_gain(key, part):
    return gain_of(key, 606).astype(jnp.bfloat16)


def draw_position_bias(key, part):
    table = 0.5 * jnp.clip(jax.random.normal(jax.random.fold_in(key, 808), (HEADS, CLIP + SEG), jnp.float32), -6.0, 6.0)
    return table.astype(jnp.bfloat16)


def shard_levels(rng, extent, shards, least, largest):
    def one(dim, shards_of):
        steps = jax.random.uniform(jax.random.fold_in(jax.random.fold_in(rng, 6), dim), (shards_of,), jnp.float32, least / len(shards), largest / len(shards))
        return jnp.repeat(jnp.exp(steps), extent[dim] // shards_of).reshape((-1,) + (1,) * (len(extent) - dim - 1))

    gain = one(*shards[0])
    for cut in shards[1:]:
        gain = gain * one(*cut)
    return gain


def gaussian(rng, extent, spread, bound, shards=(), held_as=jnp.bfloat16):
    drawn = spread * jax.random.normal(rng, extent, jnp.float32)
    if shards:
        drawn = drawn * shard_levels(rng, extent, shards, -0.22, 0.18)
    return jnp.clip(drawn, -bound, bound).astype(held_as)


def setup_inputs(seed: int = 0) -> dict:
    key_of = jax.random.split(jax.random.key(seed), 8)
    query_rows = draw_query_rows(jax.random.fold_in(key_of[7], 71), 0)
    key_rows = draw_key_rows(jax.random.fold_in(key_of[7], 71), 0)
    value_rows = gaussian(key_of[2], (SEQ, HEADS * HEAD_DIM), 1.0, 6.0, ((0, 16), (1, 2)))
    query_gain = draw_query_gain(jax.random.fold_in(key_of[7], 71), 0)
    key_gain = draw_key_gain(jax.random.fold_in(key_of[7], 71), 0)
    position_bias = draw_position_bias(jax.random.fold_in(key_of[7], 71), 0)
    output_grad = gaussian(key_of[6], (SEQ, HEADS * HEAD_DIM), 4.0, 24.0, ((0, 16), (1, 2)))
    return {"query_rows": query_rows, "key_rows": key_rows, "value_rows": value_rows, "query_gain": query_gain, "key_gain": key_gain, "position_bias": position_bias, "output_grad": output_grad}


NORM_EPS = 1e-06

def unit_rows(values):
    widened = values.astype(jnp.float32)
    scale_rows = lax.rsqrt(lax.optimization_barrier(jnp.mean(widened * widened, axis=-1, keepdims=True)) + NORM_EPS)
    return (widened * scale_rows, scale_rows)

def band_of(segments, seg_count):
    return jnp.concatenate([segments[offset:offset + seg_count] for offset in range(LEFT + 1)], axis=1)

def unband(banded, seg_count):
    summed = jnp.zeros((seg_count + LEFT, SEG) + banded.shape[2:], jnp.float32)
    for offset in range(LEFT + 1):
        summed = summed.at[offset:offset + seg_count].add(banded[:, offset * SEG:(offset + 1) * SEG])
    return summed

def layout(seg_count):
    band_pos = np.repeat(np.arange(LEFT + 1), SEG)
    key_pos = np.tile(np.arange(SEG), LEFT + 1)
    query_pos = np.arange(SEG)[:, None]
    distance = (LEFT - band_pos)[None, :] * SEG + query_pos - key_pos[None, :]
    bias_index = (np.minimum(distance, CLIP) + SEG - 1).astype(np.int32)
    visible = np.arange(seg_count)[:, None] - LEFT + band_pos[None, :] >= 0
    segs_block = TOK_DEV // SEG
    query_seg_index = np.arange(seg_count)[:, None]
    key_seg_index = query_seg_index - LEFT + band_pos[None, :]
    crossing = (query_seg_index // segs_block != key_seg_index // segs_block).astype(np.float32)
    return (bias_index, visible, crossing)

def split_unband(banded, crossing, seg_count):
    cross_mask = jnp.asarray(crossing)[:, :, None]
    own_part = unband(banded * (1.0 - cross_mask), seg_count)[LEFT:].reshape(SEQ, HEAD_DIM)
    cross_part = unband(banded * cross_mask, seg_count)[LEFT:].reshape(SEQ, HEAD_DIM)
    cross_low = lax.optimization_barrier(cross_part.astype(jnp.bfloat16)).astype(jnp.float32)
    return own_part + cross_low

def reference(query_rows, key_rows, value_rows, query_gain, key_gain, position_bias, output_grad):
    seg_count = SEQ // SEG
    bias_index, visible, crossing = layout(seg_count)
    score_scale = HEAD_DIM ** (-0.5)
    gain_query = query_gain.astype(jnp.float32)
    gain_key = key_gain.astype(jnp.float32)

    def by_head(matrix):
        return matrix.reshape(SEQ, HEADS, HEAD_DIM).transpose(1, 0, 2)

    def one_head(inputs):
        query_head, key_head, value_head, grad_head, bias_table = inputs
        query_hat, query_scale = unit_rows(query_head)
        key_hat, key_scale = unit_rows(key_head)
        query_unit = lax.optimization_barrier((query_hat * gain_query).astype(jnp.bfloat16))
        key_unit = lax.optimization_barrier((key_hat * gain_key).astype(jnp.bfloat16))
        padding = jnp.zeros((LEFT * SEG, HEAD_DIM), jnp.bfloat16)
        key_band = band_of(jnp.concatenate([padding, key_unit], 0).reshape(seg_count + LEFT, SEG, HEAD_DIM), seg_count).astype(jnp.float32)
        value_band = band_of(jnp.concatenate([padding, value_head], 0).reshape(seg_count + LEFT, SEG, HEAD_DIM), seg_count).astype(jnp.float32)
        query_seg = query_unit.reshape(seg_count, SEG, HEAD_DIM).astype(jnp.float32)
        grad_seg = grad_head.reshape(seg_count, SEG, HEAD_DIM).astype(jnp.float32)
        row_bias = bias_table.astype(jnp.float32)[bias_index]
        scores = jnp.einsum('cqd,ckd->cqk', query_seg, key_band) * score_scale + row_bias[None]
        scores = jnp.where(visible[:, None, :], scores, -jnp.inf)
        row_peak = lax.optimization_barrier(jnp.max(scores, axis=-1, keepdims=True))
        raised = jnp.exp(scores - row_peak)
        weights = raised / lax.optimization_barrier(jnp.sum(raised, axis=-1, keepdims=True))
        weights_low = lax.optimization_barrier(weights.astype(jnp.bfloat16)).astype(jnp.float32)
        d_weights = jnp.einsum('cqd,ckd->cqk', grad_seg, value_band)
        row_delta = lax.optimization_barrier(jnp.sum(weights * d_weights, axis=-1, keepdims=True))
        d_scores = weights * (d_weights - row_delta)
        d_low = lax.optimization_barrier(d_scores.astype(jnp.bfloat16)).astype(jnp.float32)
        dq_unit = (jnp.einsum('cqk,ckd->cqd', d_low, key_band) * score_scale).reshape(SEQ, HEAD_DIM)
        dk_unit = split_unband(jnp.einsum('cqk,cqd->ckd', d_low, query_seg) * score_scale, crossing, seg_count)
        value_grad = split_unband(jnp.einsum('cqk,cqd->ckd', weights_low, grad_seg), crossing, seg_count)
        bias_grad = jnp.zeros((CLIP + SEG,), jnp.float32).at[bias_index.ravel()].add(lax.optimization_barrier(jnp.sum(d_scores, axis=0)).ravel())
        dq_scaled = dq_unit * gain_query
        query_grad = query_scale * (dq_scaled - query_hat * lax.optimization_barrier(jnp.mean(dq_scaled * query_hat, axis=-1, keepdims=True)))
        dk_scaled = dk_unit * gain_key
        key_grad = key_scale * (dk_scaled - key_hat * lax.optimization_barrier(jnp.mean(dk_scaled * key_hat, axis=-1, keepdims=True)))
        return (query_grad.astype(jnp.bfloat16), key_grad.astype(jnp.bfloat16), value_grad.astype(jnp.bfloat16), bias_grad, lax.optimization_barrier(jnp.sum(dq_unit * query_hat, axis=0)), lax.optimization_barrier(jnp.sum(dk_unit * key_hat, axis=0)))
    results = lax.map(one_head, (by_head(query_rows), by_head(key_rows), by_head(value_rows), by_head(output_grad), position_bias))

    def to_rows(stacked):
        return stacked.transpose(1, 0, 2).reshape(SEQ, HEADS * HEAD_DIM)
    return (to_rows(results[0]), to_rows(results[1]), to_rows(results[2]), results[3], lax.optimization_barrier(jnp.sum(results[4], axis=0)), lax.optimization_barrier(jnp.sum(results[5], axis=0)))
```

```python
import functools

import jax
import jax.numpy as jnp
from jax import lax
from jax.experimental import pallas as pl
from jax.experimental.pallas import tpu as pltpu
from jax.sharding import PartitionSpec as P

SEG = 64
LEFT = 8
REACH = SEG * LEFT
RSPAN = 320
NORM_EPS = 1e-06
BLK = 2 * SEG
BAND = REACH + BLK
NEG = -1e30
F32 = jnp.float32
BF16 = jnp.bfloat16


def dot(a, b, dims):
    return lax.dot_general(a, b, (dims, ((), ())), preferred_element_type=F32)


def half_ones():
    row = lax.broadcasted_iota(jnp.int32, (BLK, BLK), 0) // 64
    col = lax.broadcasted_iota(jnp.int32, (BLK, BLK), 1) // 64
    return jnp.where(row == col, 1.0, 0.0).astype(BF16)


def head_mean(x, ones):
    high = x.astype(BF16)
    low = (x - high.astype(F32)).astype(BF16)
    return (dot(high, ones, ((1,), (0,))) + dot(low, ones, ((1,), (0,)))) * (1.0 / 64.0)


def normed(rows, ones):
    wide = rows.astype(F32)
    scale = lax.rsqrt(head_mean(wide * wide, ones) + NORM_EPS)
    return wide * scale, scale


def norm_grad(d_unit, gain, hat, scale, ones):
    scaled = d_unit * gain
    return scale * (scaled - hat * head_mean(scaled * hat, ones))


def stack_halves(x):
    lane = lax.broadcasted_iota(jnp.int32, x.shape, 1)
    zero = jnp.zeros_like(x)
    return jnp.concatenate([jnp.where(lane < 64, x, zero), jnp.where(lane < 64, zero, x)], axis=0)


def build_bias(table_row, bias_ref, head):
    wide = jnp.broadcast_to(table_row, (8, 512))
    sub = lax.broadcasted_iota(jnp.int32, (8, 512), 0)
    for bit in (1, 2, 4):
        wide = jnp.where((sub & bit) != 0, pltpu.roll(wide, bit, 1), wide)
    half = 8
    while half < BLK:
        wide = jnp.concatenate([wide, pltpu.roll(wide, half, 1)], axis=0)
        half *= 2
    lanes = slice(head * BLK, (head + 1) * BLK)
    row = lax.broadcasted_iota(jnp.int32, (BLK, BLK), 0)
    col = lax.broadcasted_iota(jnp.int32, (BLK, BLK), 1)
    far = jnp.broadcast_to(table_row[:, 0:1], (BLK, BLK))
    bias_ref[0:BLK, lanes] = jnp.where((row < SEG) & (col >= SEG), NEG, far)
    bias_ref[BLK : 2 * BLK, lanes] = far
    for j in range(3):
        tile = wide[:, ((4 - j) % 4) * BLK : ((4 - j) % 4) * BLK + BLK]
        if j == 2:
            tile = jnp.where((row >= SEG) & (col < SEG), NEG, tile)
        bias_ref[(2 + j) * BLK : (3 + j) * BLK, lanes] = tile


def fold_bias(acc_ref, head):
    lanes = slice(head * BLK, (head + 1) * BLK)
    tiles = [acc_ref[j * BLK : (j + 1) * BLK, lanes] for j in range(3)]
    wide = jnp.concatenate([tiles[0], jnp.zeros_like(tiles[0]), tiles[2], tiles[1]], axis=1)
    half = BLK // 2
    while half >= 8:
        wide = wide[:half] + pltpu.roll(wide[half:], 512 - half, 1)
        half //= 2
    for half in (4, 2, 1):
        wide = wide + pltpu.roll(pltpu.roll(wide, 512 - half, 1), 8 - half, 0)
    return wide[0:1]


def rounds_of(size):
    rounds, stride = [], 1
    while stride < size:
        radix = 4 if size // stride % 4 == 0 else 2
        rounds.append((stride, radix))
        stride *= radix
    return rounds


def peer(index, stride, radix, step):
    digit = (index // stride) % radix
    return index + stride * ((digit + step) % radix - digit)


def ring_sum(parts):
    if len(parts) == 4:
        return (parts[0] + parts[2]) + (parts[1] + parts[3])
    return parts[0] + parts[1] if len(parts) == 2 else parts[0]


def kernel(
    sp, tp, q_hbm, k_hbm, v_hbm, g_hbm, qgain_hbm, kgain_hbm, table_hbm,
    qg_ref, kg_ref, vg_ref, out_ref,
    q_ref, k_ref, v_ref, g_ref,
    k_s, kt_s, v_s, bias_s, acc_s, s_s, dw_s, ds_s, w_s, qs_s, gs_s, hat_s, scale_s, dk_s, dv_s, clip_s, gq_s, gk_s,
    pk_s, pv_s, ck_s, cv_s, bk_s, bv_s, bsum_s, bgot_s, gsum_s, ggot_s, gfirst_s,
    qgain_s, kgain_s, raw_s, wide_s, table_s, gains_s,
    prior_send, prior_recv, cross_send, cross_recv, bias_send, bias_recv, gain_send, gain_recv, load_sem, small_sem,
):
    tokens = q_ref.shape[0]
    blocks = tokens // BLK
    pairs = pk_s.shape[0]
    me = lax.axis_index("sp")
    me_tp = lax.axis_index("tp")
    right, left = lax.rem(me + 1, sp), lax.rem(me + sp - 1, sp)
    rounds = rounds_of(sp)
    count = len(rounds)
    peers = [[{"sp": peer(me, stride, radix, k)} for k in range(1, radix)] for stride, radix in rounds]
    combos = [(k, t) for k in range(rounds[0][1]) for t in range(tp) if k or t]
    nearby = [{"sp": peer(me, 1, rounds[0][1], k), "tp": lax.rem(me_tp + t, tp)} for k, t in combos]
    first, last = me == 0, me == sp - 1

    def lanes_of(p):
        return pl.ds(pl.multiple_of(p * BLK, BLK), BLK)

    def loads(p):
        moves = ((k_hbm, k_ref), (q_hbm, q_ref), (v_hbm, v_ref), (g_hbm, g_ref))
        return [
            pltpu.make_async_copy(src.at[:, lanes_of(p)], dst.at[:, lanes_of(p)], load_sem.at[n, p])
            for n, (src, dst) in enumerate(moves)
        ]

    smalls = [
        pltpu.make_async_copy(src, dst, small_sem.at[n])
        for n, (src, dst) in enumerate(((qgain_hbm, qgain_s), (kgain_hbm, kgain_s), (table_hbm, raw_s)))
    ]
    for copy in smalls:
        copy.start()
    for p in range(pairs):
        for copy in loads(p):
            copy.start()

    barrier = pltpu.get_barrier_semaphore()
    greeted = [{"sp": right}, {"sp": left}] + nearby + [device for group in peers for device in group]
    for device in greeted:
        pl.semaphore_signal(barrier, inc=1, device_id=device, device_id_type=pl.DeviceIdType.MESH)
    pl.semaphore_wait(barrier, len(greeted))

    def remote(src, dst, send, recv, device):
        return pltpu.make_async_remote_copy(
            src_ref=src, dst_ref=dst, send_sem=send, recv_sem=recv,
            device_id=device, device_id_type=pl.DeviceIdType.MESH,
        )

    def prior_copies(p):
        rows = slice(tokens - REACH, tokens)
        return (
            remote(k_hbm.at[rows, lanes_of(p)], pk_s.at[p], prior_send.at[0, p], prior_recv.at[0, p], {"sp": right}),
            remote(v_hbm.at[rows, lanes_of(p)], pv_s.at[p], prior_send.at[1, p], prior_recv.at[1, p], {"sp": right}),
        )

    def cross_copies(p):
        return (
            remote(ck_s.at[p], bk_s.at[p], cross_send.at[0, p], cross_recv.at[0, p], {"sp": left}),
            remote(cv_s.at[p], bv_s.at[p], cross_send.at[1, p], cross_recv.at[1, p], {"sp": left}),
        )

    @pl.when(jnp.logical_not(last))
    def _():
        for p in range(pairs):
            for copy in prior_copies(p):
                copy.start()

    @pl.when(first)
    def _():
        pk_s[...] = jnp.zeros_like(pk_s)
        pv_s[...] = jnp.zeros_like(pv_s)

    @pl.when(last)
    def _():
        bk_s[...] = jnp.zeros_like(bk_s)
        bv_s[...] = jnp.zeros_like(bv_s)

    def bias_copies(r, p):
        return [
            remote(bsum_s.at[r, p], bgot_s.at[r, p, k], bias_send.at[r, k, p], bias_recv.at[r, k, p], device)
            for k, device in enumerate(peers[r])
        ]

    def bias_start(r, p):
        for copy in bias_copies(r, p):
            copy.start()

    def bias_add(r, p):
        for copy in bias_copies(r, p):
            copy.wait_recv()
        bsum_s[r + 1, p] = ring_sum([bsum_s[r, p]] + [bgot_s[r, p, k] for k in range(len(peers[r]))])

    def bias_step(r, p):
        bias_add(r - 1, p)
        if r < count:
            bias_start(r, p)

    def gain_copies(r):
        if r == 0:
            return [
                remote(gsum_s.at[0], gfirst_s.at[n], gain_send.at[0, n], gain_recv.at[0, n], device)
                for n, device in enumerate(nearby)
            ]
        return [
            remote(gsum_s.at[r], ggot_s.at[r, k], gain_send.at[r, k], gain_recv.at[r, k], device)
            for k, device in enumerate(peers[r])
        ]

    def gain_start(r):
        for copy in gain_copies(r):
            copy.start()

    def gain_add(r):
        for copy in gain_copies(r):
            copy.wait_recv()
        if r == 0:
            parts = {combo: gfirst_s[n] for n, combo in enumerate(combos)}
            parts[0, 0] = gsum_s[0]
            gsum_s[1] = ring_sum([ring_sum([parts[k, t] for t in range(tp)]) for k in range(rounds[0][1])])
        else:
            gsum_s[r + 1] = ring_sum([gsum_s[r]] + [ggot_s[r, k] for k in range(len(peers[r]))])

    ones = half_ones()
    for copy in smalls:
        copy.wait()
    for half in range(2):
        gains_s[0:1, half * 64 : half * 64 + 64] = qgain_s[...].astype(F32)
        gains_s[1:2, half * 64 : half * 64 + 64] = kgain_s[...].astype(F32)
    gain_q = gains_s[0:1, :]
    gain_k = gains_s[1:2, :]
    heads, span = raw_s.shape
    wide_s[...] = jnp.zeros_like(wide_s)
    wide_s[0:heads, 0:span] = raw_s[...].astype(F32)
    wide = wide_s[...]
    place = lax.broadcasted_iota(jnp.int32, wide.shape, 1)
    moved = pltpu.roll(wide, 193, 1)
    table_s[...] = jnp.where(place <= 128, wide[:, span - 1 : span], jnp.where(place < 193, NEG, moved))
    gq_s[...] = jnp.zeros_like(gq_s)
    gk_s[...] = jnp.zeros_like(gk_s)

    def key_tile(raw, b):
        unit = normed(raw, ones)[0] * gain_k
        k_s[b * BLK : (b + 1) * BLK, :] = unit.astype(BF16)
        kt_s[:, b * BLK : (b + 1) * BLK] = unit.T.astype(BF16)

    def finish(p):
        slot = lax.rem(p, 2)
        @pl.when(jnp.logical_not(last))
        def _():
            for copy in cross_copies(p):
                copy.wait_recv()

        total = jnp.zeros((1, BLK), F32)
        for b in range(blocks):
            rows = slice(b * BLK, (b + 1) * BLK)
            hat, scale = normed(k_ref[rows, lanes_of(p)], ones)
            ext = slice(REACH + b * BLK, REACH + (b + 1) * BLK)
            dk, dv = dk_s[slot, ext, :], dv_s[slot, ext, :]
            back = b * BLK - (tokens - REACH)
            if back >= 0:
                dk = dk + bk_s[p, back : back + BLK, :].astype(F32)
                dv = dv + bv_s[p, back : back + BLK, :].astype(F32)
            total = total + jnp.sum(dk * hat, axis=0, keepdims=True)
            kg_ref[rows, lanes_of(p)] = norm_grad(dk, gain_k, hat, scale, ones).astype(BF16)
            vg_ref[rows, lanes_of(p)] = dv.astype(BF16)
        gk_s[...] += total

    def pair(p, _):
        slot = lax.rem(p, 2)
        for head in range(2):
            build_bias(table_s[pl.ds(p * 2 + head, 1), :], bias_s, head)
        dk_s[slot] = jnp.zeros(dk_s.shape[1:], F32)
        dv_s[slot] = jnp.zeros(dv_s.shape[1:], F32)
        acc_s[...] = jnp.zeros_like(acc_s)
        clip_s[...] = jnp.zeros_like(clip_s)
        for copy in loads(p):
            copy.wait()
        for b in range(blocks):
            rows = slice(b * BLK, (b + 1) * BLK)
            key_tile(k_ref[rows, lanes_of(p)], b + LEFT // 2)
            hat, scale = normed(q_ref[rows, lanes_of(p)], ones)
            hat_s[rows, :] = hat
            scale_s[rows, :] = scale
            qs_s[b] = stack_halves((hat * gain_q).astype(BF16) * jnp.asarray(0.125, BF16))
            gs_s[b] = stack_halves(g_ref[rows, lanes_of(p)])
        v_s[REACH:, :] = v_ref[:, lanes_of(p)]
        @pl.when(jnp.logical_not(first))
        def _():
            for copy in prior_copies(p):
                copy.wait_recv()

        for b in range(LEFT // 2):
            key_tile(pk_s[p, b * BLK : (b + 1) * BLK, :], b)
        v_s[:REACH, :] = pv_s[p]

        def tile(j):
            return slice(j * BLK, (j + 1) * BLK)

        def score(i, j, peaks):
            keys = tile(i + j)
            s = dot(k_s[keys, :], qs_s[i], ((1,), (1,))) + bias_s[tile(j), :]
            s_s[i % 2, tile(j), :] = s
            dw_s[i % 2, tile(j), :] = dot(v_s[keys, :], gs_s[i], ((1,), (1,)))
            top = jnp.max(s, axis=0, keepdims=True)
            peaks.append(top + penalty if j < LEFT // 2 - i else top)

        def product(i, j):
            keys = tile(i + j)
            dk_s[slot, keys, :] += dot(ds_s[i % 2, tile(j), :], qs_s[i], ((1,), (0,)))
            dv_s[slot, keys, :] += dot(w_s[i % 2, tile(j), :], gs_s[i], ((1,), (0,)))

        def query_side(i):
            rows = tile(i)
            dqt = dot(kt_s[:, i * BLK : i * BLK + BAND], ds_s[i % 2], ((1,), (0,)))
            dqt = jnp.concatenate([dqt[:64, :BLK], dqt[64:, BLK:]], axis=0)
            dq = dqt.T * 0.125
            hat = hat_s[rows, :]
            gq_s[...] += jnp.sum(dq * hat, axis=0, keepdims=True)
            qg_ref[rows, lanes_of(p)] = norm_grad(dq, gain_q, hat, scale_s[rows, :], ones).astype(BF16)

        penalty = jnp.where(first, NEG, 0.0)
        peaks = {}
        for step in range(blocks + 2):
            ahead, here, behind = step, step - 1, step - 2
            peaks[ahead] = []
            if 0 <= here < blocks:
                peak = functools.reduce(jnp.maximum, peaks[here])
                total = jnp.zeros((1, 2 * BLK), F32)
                delta = jnp.zeros((1, 2 * BLK), F32)
                clipped = jnp.zeros((1, 2 * BLK), F32)
            for j in range(5):
                if ahead < blocks:
                    score(ahead, j, peaks[ahead])
                if 0 <= here < blocks:
                    e = jnp.exp(s_s[here % 2, tile(j), :] - (peak - penalty if j < LEFT // 2 - here else peak))
                    s_s[here % 2, tile(j), :] = e
                    total = total + jnp.sum(e, axis=0, keepdims=True)
                    delta = delta + jnp.sum(e * dw_s[here % 2, tile(j), :], axis=0, keepdims=True)
            if 0 <= here < blocks:
                inverse = 1.0 / total
                delta = delta * inverse
            if behind >= 0:
                query_side(behind)
            for j in range(5):
                if behind >= 0:
                    product(behind, j)
                if 0 <= here < blocks:
                    w = s_s[here % 2, tile(j), :] * inverse
                    ds = w * (dw_s[here % 2, tile(j), :] - delta)
                    if j < 2:
                        clipped = clipped + jnp.sum(ds, axis=0, keepdims=True)
                    else:
                        acc_s[tile(j - 2), :] += ds
                    ds_s[here % 2, tile(j), :] = ds.astype(BF16)
                    w_s[here % 2, tile(j), :] = w.astype(BF16)
            if 0 <= here < blocks:
                clip_s[...] += clipped
        ck_s[p] = dk_s[slot, :REACH, :].astype(BF16)
        cv_s[p] = dv_s[slot, :REACH, :].astype(BF16)
        @pl.when(jnp.logical_not(first))
        def _():
            for copy in cross_copies(p):
                copy.start()

        lane = lax.broadcasted_iota(jnp.int32, (1, 512), 1)
        rows = []
        for head in range(2):
            far = jnp.sum(clip_s[:, head * BLK : (head + 1) * BLK], axis=1, keepdims=True)
            row = fold_bias(acc_s, head) + jnp.where(lane == 0, far, 0.0)
            rows += [row[:, b * BLK : (b + 1) * BLK] for b in range(4)]
        bsum_s[0, p] = jnp.concatenate(rows, axis=0)
        bias_start(0, p)
        for r in range(1, count + 1):

            @pl.when(p >= r)
            def _():
                bias_step(r, p - r)

        @pl.when(p > 0)
        def _():
            finish(p - 1)

        return 0

    lax.fori_loop(0, pairs, pair, 0)
    finish(pairs - 1)
    gsum_s[0] = jnp.zeros(gsum_s.shape[1:], F32)
    gsum_s[0, 0:1, :] = gq_s[...]
    gsum_s[0, 1:2, :] = gk_s[...]
    gain_start(0)
    for t in range(count):
        for r in range(1, count + 1):
            if 0 <= pairs + t - r < pairs:
                bias_step(r, pairs + t - r)
        gain_add(t)
        if t + 1 < count:
            gain_start(t + 1)
    for p in range(pairs):
        out_ref[p] = bsum_s[count, p]
    out_ref[pairs] = gsum_s[count]

    @pl.when(jnp.logical_not(last))
    def _():
        for p in range(pairs):
            for copy in prior_copies(p):
                copy.wait_send()

    @pl.when(jnp.logical_not(first))
    def _():
        for p in range(pairs):
            for copy in cross_copies(p):
                copy.wait_send()

    for r in range(count):
        for p in range(pairs):
            for copy in bias_copies(r, p):
                copy.wait_send()
        for copy in gain_copies(r):
            copy.wait_send()


def drain(
    qg_ref, kg_ref, vg_ref, stat_ref, qg_hbm, kg_hbm, vg_hbm, bias_hbm, gq_hbm, gk_hbm,
    wide_s, bias_s, gq_s, gk_s, sem,
):
    moves = [(qg_ref, qg_hbm), (kg_ref, kg_hbm), (vg_ref, vg_hbm), (gq_s, gq_hbm), (gk_s, gk_hbm), (bias_s, bias_hbm)]
    copies = [pltpu.make_async_copy(src, dst, sem.at[n]) for n, (src, dst) in enumerate(moves)]
    for copy in copies[:3]:
        copy.start()
    heads, span = bias_s.shape
    pairs = heads // 2
    for row, ref in enumerate((gq_s, gk_s)):
        both = stat_ref[pairs, row : row + 1, :]
        ref[...] = (both + pltpu.roll(both, 64, 1))[:, :64].reshape(64)
    copies[3].start()
    copies[4].start()
    wide_s[...] = jnp.zeros_like(wide_s)
    for head in range(heads):
        for b in range(4):
            row = head % 2 * 4 + b
            wide_s[head : head + 1, b * BLK : (b + 1) * BLK] = stat_ref[head // 2, row : row + 1, :]
    wide = wide_s[...]
    lane = lax.broadcasted_iota(jnp.int32, wide.shape, 1)
    far = jnp.sum(jnp.where(lane <= 128, wide, 0.0), axis=1, keepdims=True)
    folded = jnp.where(lane == span - 1, far, pltpu.roll(wide, 319, 1))
    bias_s[...] = folded[:heads, :span]
    copies[5].start()
    for copy in copies:
        copy.wait()


def body(query_rows, key_rows, value_rows, query_gain, key_gain, position_bias, output_grad):
    heads = position_bias.shape[0]
    pairs = heads // 2
    tokens = query_rows.shape[0]
    sp, tp = lax.axis_size("sp"), lax.axis_size("tp")
    count = len(rounds_of(sp))
    group = 4 * tp
    ext = tokens + REACH
    padded = (heads + 7) // 8 * 8
    vmem, hbm = pl.BlockSpec(memory_space=pltpu.VMEM), pl.BlockSpec(memory_space=pltpu.HBM)
    shape = jax.ShapeDtypeStruct
    grads = shape((tokens, heads * 64), BF16)
    sems = pltpu.SemaphoreType.DMA
    operands = (
        query_rows, key_rows, value_rows, output_grad,
        query_gain.reshape(1, 64), key_gain.reshape(1, 64), position_bias,
    )
    results = pl.pallas_call(
        functools.partial(kernel, sp, tp),
        in_specs=[hbm] * 7,
        out_specs=[vmem] * 4,
        out_shape=[grads, grads, grads, shape((pairs + 1, 8, BLK), F32)],
        scratch_shapes=[pltpu.VMEM((tokens, heads * 64), BF16)] * 4
        + [
            pltpu.VMEM((ext, BLK), BF16), pltpu.VMEM((BLK, ext), BF16), pltpu.VMEM((ext, BLK), BF16),
            pltpu.VMEM((BAND, 2 * BLK), F32), pltpu.VMEM((3 * BLK, 2 * BLK), F32),
            pltpu.VMEM((2, BAND, 2 * BLK), F32), pltpu.VMEM((2, BAND, 2 * BLK), F32),
            pltpu.VMEM((2, BAND, 2 * BLK), BF16), pltpu.VMEM((2, BAND, 2 * BLK), BF16),
            pltpu.VMEM((tokens // BLK, 2 * BLK, BLK), BF16), pltpu.VMEM((tokens // BLK, 2 * BLK, BLK), BF16),
            pltpu.VMEM((tokens, BLK), F32), pltpu.VMEM((tokens, BLK), F32),
            pltpu.VMEM((2, ext, BLK), F32), pltpu.VMEM((2, ext, BLK), F32),
            pltpu.VMEM((1, 2 * BLK), F32), pltpu.VMEM((1, BLK), F32), pltpu.VMEM((1, BLK), F32),
        ]
        + [pltpu.VMEM((pairs, REACH, BLK), BF16)] * 6
        + [
            pltpu.VMEM((count + 1, pairs, 8, BLK), F32), pltpu.VMEM((count, pairs, 3, 8, BLK), F32),
            pltpu.VMEM((count + 1, 8, BLK), F32), pltpu.VMEM((count, 3, 8, BLK), F32), pltpu.VMEM((group, 8, BLK), F32),
            pltpu.VMEM((1, 64), BF16), pltpu.VMEM((1, 64), BF16), pltpu.VMEM(position_bias.shape, BF16),
            pltpu.VMEM((padded, 512), F32), pltpu.VMEM((padded, 512), F32), pltpu.VMEM((8, BLK), F32),
            sems((2, pairs)), sems((2, pairs)), sems((2, pairs)), sems((2, pairs)),
            sems((count, 3, pairs)), sems((count, 3, pairs)), sems((count, group)), sems((count, group)),
            sems((4, pairs)), sems((3,)),
        ],
        compiler_params=pltpu.CompilerParams(collective_id=0, has_side_effects=True, vmem_limit_bytes=48 << 20),
        name="attend",
    )(*[pltpu.with_memory_space_constraint(x, pltpu.HBM) for x in operands])
    return pl.pallas_call(
        drain,
        in_specs=[vmem] * 4,
        out_specs=[hbm] * 6,
        out_shape=[grads, grads, grads, shape(position_bias.shape, F32), shape((64,), F32), shape((64,), F32)],
        scratch_shapes=[
            pltpu.VMEM((padded, 512), F32), pltpu.VMEM(position_bias.shape, F32),
            pltpu.VMEM((64,), F32), pltpu.VMEM((64,), F32), sems((6,)),
        ],
        compiler_params=pltpu.CompilerParams(vmem_limit_bytes=2 << 20),
        name="drain",
    )(*results)


def solution(mesh):
    placed = (P("sp", "tp"), P("sp", "tp"), P("sp", "tp"), P(), P(), P("tp", None), P("sp", "tp"))
    return jax.shard_map(
        body,
        mesh=mesh,
        in_specs=placed,
        out_specs=(P("sp", "tp"), P("sp", "tp"), P("sp", "tp"), P("tp", None), P(), P()),
        check_vma=False,
    )
```

```python
import functools

import jax
import jax.numpy as jnp
from jax import lax
from jax.experimental import pallas as pl
from jax.experimental.pallas import tpu as pltpu
from jax.sharding import PartitionSpec as P

SEG = 64
LEFT = 8
REACH = SEG * LEFT
RSPAN = 320
NORM_EPS = 1e-06
BLK = 2 * SEG
BAND = REACH + BLK
NEG = -1e30
LAG = 3
F32 = jnp.float32
BF16 = jnp.bfloat16


def dot(a, b, dims):
    return lax.dot_general(a, b, (dims, ((), ())), preferred_element_type=F32)


def half_ones():
    row = lax.broadcasted_iota(jnp.int32, (BLK, BLK), 0) // 64
    col = lax.broadcasted_iota(jnp.int32, (BLK, BLK), 1) // 64
    return jnp.where(row == col, 1.0, 0.0).astype(BF16)


def head_mean(x, ones):
    high = x.astype(BF16)
    low = (x - high.astype(F32)).astype(BF16)
    return (dot(high, ones, ((1,), (0,))) + dot(low, ones, ((1,), (0,)))) * (1.0 / 64.0)


def normed(rows, ones):
    wide = rows.astype(F32)
    scale = lax.rsqrt(head_mean(wide * wide, ones) + NORM_EPS)
    return wide * scale, scale


def norm_grad(d_unit, gain, hat, scale, ones):
    scaled = d_unit * gain
    return scale * (scaled - hat * head_mean(scaled * hat, ones))


def stack_halves(x):
    lane = lax.broadcasted_iota(jnp.int32, x.shape, 1)
    zero = jnp.zeros_like(x)
    return jnp.concatenate([jnp.where(lane < 64, x, zero), jnp.where(lane < 64, zero, x)], axis=0)


def build_bias(table_row, bias_ref, head):
    wide = jnp.broadcast_to(table_row, (8, 512))
    sub = lax.broadcasted_iota(jnp.int32, (8, 512), 0)
    for bit in (1, 2, 4):
        wide = jnp.where((sub & bit) != 0, pltpu.roll(wide, bit, 1), wide)
    half = 8
    while half < BLK:
        wide = jnp.concatenate([wide, pltpu.roll(wide, half, 1)], axis=0)
        half *= 2
    lanes = slice(head * BLK, (head + 1) * BLK)
    row = lax.broadcasted_iota(jnp.int32, (BLK, BLK), 0)
    col = lax.broadcasted_iota(jnp.int32, (BLK, BLK), 1)
    far = jnp.broadcast_to(table_row[:, 0:1], (BLK, BLK))
    bias_ref[0:BLK, lanes] = jnp.where((row < SEG) & (col >= SEG), NEG, far)
    bias_ref[BLK : 2 * BLK, lanes] = far
    for j in range(3):
        tile = wide[:, ((4 - j) % 4) * BLK : ((4 - j) % 4) * BLK + BLK]
        if j == 2:
            tile = jnp.where((row >= SEG) & (col < SEG), NEG, tile)
        bias_ref[(2 + j) * BLK : (3 + j) * BLK, lanes] = tile


def fold_bias(acc_ref, head):
    lanes = slice(head * BLK, (head + 1) * BLK)
    tiles = [acc_ref[j * BLK : (j + 1) * BLK, lanes] for j in range(3)]
    wide = jnp.concatenate([tiles[0], jnp.zeros_like(tiles[0]), tiles[2], tiles[1]], axis=1)
    half = BLK // 2
    while half >= 8:
        wide = wide[:half] + pltpu.roll(wide[half:], 512 - half, 1)
        half //= 2
    for half in (4, 2, 1):
        wide = wide + pltpu.roll(pltpu.roll(wide, 512 - half, 1), 8 - half, 0)
    return wide[0:1]


def rounds_of(size):
    rounds, stride = [], 1
    while stride < size:
        radix = 4 if size // stride % 4 == 0 else 2
        rounds.append((stride, radix))
        stride *= radix
    return rounds


def peer(index, stride, radix, step):
    digit = (index // stride) % radix
    return index + stride * ((digit + step) % radix - digit)


def ring_sum(parts):
    if len(parts) == 4:
        return (parts[0] + parts[2]) + (parts[1] + parts[3])
    return parts[0] + parts[1] if len(parts) == 2 else parts[0]


def kernel(
    sp, tp, q_hbm, k_hbm, v_hbm, g_hbm, qgain_hbm, kgain_hbm, table_hbm,
    qg_ref, kg_ref, vg_ref, out_ref,
    q_ref, k_ref, v_ref, g_ref,
    khat_s, k_s, kt_s, v_s, bias_s, acc_s, s_s, dw_s, ds_s, w_s, qs_s, gs_s, hat_s, scale_s, dk_s, dv_s, clip_s, gq_s, gk_s,
    pk_s, pv_s, ck_s, cv_s, bk_s, bv_s, bsum_s, bgot_s, gsum_s, ggot_s, gfirst_s,
    qgain_s, kgain_s, raw_s, wide_s, table_s, gains_s,
    prior_send, prior_recv, cross_send, cross_recv, bias_send, bias_recv, gain_send, gain_recv, load_sem, small_sem,
):
    tokens = q_ref.shape[0]
    blocks = tokens // BLK
    pairs = pk_s.shape[0]
    me = lax.axis_index("sp")
    me_tp = lax.axis_index("tp")
    right, left = lax.rem(me + 1, sp), lax.rem(me + sp - 1, sp)
    rounds = rounds_of(sp)
    count = len(rounds)
    peers = [[{"sp": peer(me, stride, radix, k)} for k in range(1, radix)] for stride, radix in rounds]
    combos = [(k, t) for k in range(rounds[0][1]) for t in range(tp) if k or t]
    nearby = [{"sp": peer(me, 1, rounds[0][1], k), "tp": lax.rem(me_tp + t, tp)} for k, t in combos]
    first, last = me == 0, me == sp - 1

    def lanes_of(p):
        return pl.ds(pl.multiple_of(p * BLK, BLK), BLK)

    def loads(p):
        moves = ((k_hbm, k_ref), (q_hbm, q_ref), (v_hbm, v_ref), (g_hbm, g_ref))
        return [
            pltpu.make_async_copy(src.at[:, lanes_of(p)], dst.at[:, lanes_of(p)], load_sem.at[n, p])
            for n, (src, dst) in enumerate(moves)
        ]

    smalls = [
        pltpu.make_async_copy(src, dst, small_sem.at[n])
        for n, (src, dst) in enumerate(((qgain_hbm, qgain_s), (kgain_hbm, kgain_s), (table_hbm, raw_s)))
    ]
    for copy in smalls:
        copy.start()
    for p in range(pairs):
        for copy in loads(p):
            copy.start()

    barrier = pltpu.get_barrier_semaphore()
    greeted = [{"sp": right}, {"sp": left}] + nearby + [device for group in peers for device in group]
    for device in greeted:
        pl.semaphore_signal(barrier, inc=1, device_id=device, device_id_type=pl.DeviceIdType.MESH)
    pl.semaphore_wait(barrier, len(greeted))

    def remote(src, dst, send, recv, device):
        return pltpu.make_async_remote_copy(
            src_ref=src, dst_ref=dst, send_sem=send, recv_sem=recv,
            device_id=device, device_id_type=pl.DeviceIdType.MESH,
        )

    def prior_copies(p):
        rows = slice(tokens - REACH, tokens)
        return (
            remote(k_hbm.at[rows, lanes_of(p)], pk_s.at[p], prior_send.at[0, p], prior_recv.at[0, p], {"sp": right}),
            remote(v_hbm.at[rows, lanes_of(p)], pv_s.at[p], prior_send.at[1, p], prior_recv.at[1, p], {"sp": right}),
        )

    def cross_copies(p):
        return (
            remote(ck_s.at[p], bk_s.at[p], cross_send.at[0, p], cross_recv.at[0, p], {"sp": left}),
            remote(cv_s.at[p], bv_s.at[p], cross_send.at[1, p], cross_recv.at[1, p], {"sp": left}),
        )

    @pl.when(jnp.logical_not(last))
    def _():
        for p in range(pairs):
            for copy in prior_copies(p):
                copy.start()

    @pl.when(first)
    def _():
        pk_s[...] = jnp.zeros_like(pk_s)
        pv_s[...] = jnp.zeros_like(pv_s)

    @pl.when(last)
    def _():
        bk_s[...] = jnp.zeros_like(bk_s)
        bv_s[...] = jnp.zeros_like(bv_s)

    def bias_copies(p):
        return [
            remote(bsum_s.at[0, p], bgot_s.at[0, k, p], bias_send.at[0, k, p], bias_recv.at[0, k, p], device)
            for k, device in enumerate(peers[0])
        ]

    def late_copies(r):
        return [
            remote(bsum_s.at[r], bgot_s.at[r, k], bias_send.at[r, k, 0], bias_recv.at[r, k, 0], device)
            for k, device in enumerate(peers[r])
        ]

    def bias_add(r):
        for copy in [copy for p in range(pairs) for copy in bias_copies(p)] if r == 0 else late_copies(r):
            copy.wait_recv()
        bsum_s[r + 1] = ring_sum([bsum_s[r]] + [bgot_s[r, k] for k in range(len(peers[r]))])

    def gain_copies(r):
        if r == 0:
            return [
                remote(gsum_s.at[0], gfirst_s.at[n], gain_send.at[0, n], gain_recv.at[0, n], device)
                for n, device in enumerate(nearby)
            ]
        return [
            remote(gsum_s.at[r], ggot_s.at[r, k], gain_send.at[r, k], gain_recv.at[r, k], device)
            for k, device in enumerate(peers[r])
        ]

    def gain_start(r):
        for copy in gain_copies(r):
            copy.start()

    def gain_add(r):
        for copy in gain_copies(r):
            copy.wait_recv()
        if r == 0:
            parts = {combo: gfirst_s[n] for n, combo in enumerate(combos)}
            parts[0, 0] = gsum_s[0]
            gsum_s[1] = ring_sum([ring_sum([parts[k, t] for t in range(tp)]) for k in range(rounds[0][1])])
        else:
            gsum_s[r + 1] = ring_sum([gsum_s[r]] + [ggot_s[r, k] for k in range(len(peers[r]))])

    ones = half_ones()
    for copy in smalls:
        copy.wait()
    for half in range(2):
        gains_s[0:1, half * 64 : half * 64 + 64] = qgain_s[...].astype(F32)
        gains_s[1:2, half * 64 : half * 64 + 64] = kgain_s[...].astype(F32)
    gain_q = gains_s[0:1, :]
    gain_k = gains_s[1:2, :]
    heads, span = raw_s.shape
    wide_s[...] = jnp.zeros_like(wide_s)
    wide_s[0:heads, 0:span] = raw_s[...].astype(F32)
    wide = wide_s[...]
    place = lax.broadcasted_iota(jnp.int32, wide.shape, 1)
    moved = pltpu.roll(wide, 193, 1)
    table_s[...] = jnp.where(place <= 128, wide[:, span - 1 : span], jnp.where(place < 193, NEG, moved))
    gq_s[...] = jnp.zeros_like(gq_s)
    gk_s[...] = jnp.zeros_like(gk_s)

    def key_tile(raw, b):
        hat = normed(raw, ones)[0]
        khat_s[b * BLK : (b + 1) * BLK, :] = hat
        unit = hat * gain_k
        k_s[b * BLK : (b + 1) * BLK, :] = unit.astype(BF16)
        kt_s[:, b * BLK : (b + 1) * BLK] = unit.T.astype(BF16)

    def finish(p, _):
        @pl.when(jnp.logical_not(last))
        def _():
            for copy in cross_copies(p):
                copy.wait_recv()

        for b in range(blocks):
            rows = slice(b * BLK, (b + 1) * BLK)
            hat, scale = normed(k_ref[rows, lanes_of(p)], ones)
            ext = slice(REACH + b * BLK, REACH + (b + 1) * BLK)
            dk, dv = dk_s[p, ext, :], dv_s[p, ext, :]
            back = b * BLK - (tokens - REACH)
            if back >= 0:
                dk = dk + bk_s[p, back : back + BLK, :].astype(F32)
                dv = dv + bv_s[p, back : back + BLK, :].astype(F32)
            kg_ref[rows, lanes_of(p)] = norm_grad(dk, gain_k, hat, scale, ones).astype(BF16)
            vg_ref[rows, lanes_of(p)] = dv.astype(BF16)
        return 0

    def pair(p, _):
        slot = p
        for head in range(2):
            build_bias(table_s[pl.ds(p * 2 + head, 1), :], bias_s, head)
        dk_s[slot] = jnp.zeros(dk_s.shape[1:], F32)
        dv_s[slot] = jnp.zeros(dv_s.shape[1:], F32)
        acc_s[...] = jnp.zeros_like(acc_s)
        clip_s[...] = jnp.zeros_like(clip_s)
        for copy in loads(p):
            copy.wait()
        for b in range(blocks):
            rows = slice(b * BLK, (b + 1) * BLK)
            key_tile(k_ref[rows, lanes_of(p)], b + LEFT // 2)
            hat, scale = normed(q_ref[rows, lanes_of(p)], ones)
            hat_s[rows, :] = hat
            scale_s[rows, :] = scale
            qs_s[b] = stack_halves((hat * gain_q).astype(BF16) * jnp.asarray(0.125, BF16))
            gs_s[b] = stack_halves(g_ref[rows, lanes_of(p)])
        v_s[REACH:, :] = v_ref[:, lanes_of(p)]
        @pl.when(jnp.logical_not(first))
        def _():
            for copy in prior_copies(p):
                copy.wait_recv()

        for b in range(LEFT // 2):
            key_tile(pk_s[p, b * BLK : (b + 1) * BLK, :], b)
        v_s[:REACH, :] = pv_s[p]

        def tile(j):
            return slice(j * BLK, (j + 1) * BLK)

        def score(i, j, peaks):
            keys = tile(i + j)
            s = dot(k_s[keys, :], qs_s[i], ((1,), (1,))) + bias_s[tile(j), :]
            s_s[i % 2, tile(j), :] = s
            dw_s[i % 2, tile(j), :] = dot(v_s[keys, :], gs_s[i], ((1,), (1,)))
            top = jnp.max(s, axis=0, keepdims=True)
            peaks.append(top + penalty if j < LEFT // 2 - i else top)

        def product(i, j):
            keys = tile(i + j)
            dk_s[slot, keys, :] += dot(ds_s[i % 2, tile(j), :], qs_s[i], ((1,), (0,)))
            dv_s[slot, keys, :] += dot(w_s[i % 2, tile(j), :], gs_s[i], ((1,), (0,)))

        def query_side(i):
            rows = tile(i)
            dqt = dot(kt_s[:, i * BLK : i * BLK + BAND], ds_s[i % 2], ((1,), (0,)))
            dqt = jnp.concatenate([dqt[:64, :BLK], dqt[64:, BLK:]], axis=0)
            dq = dqt.T * 0.125
            hat = hat_s[rows, :]
            gq_s[...] += jnp.sum(dq * hat, axis=0, keepdims=True)
            qg_ref[rows, lanes_of(p)] = norm_grad(dq, gain_q, hat, scale_s[rows, :], ones).astype(BF16)

        penalty = jnp.where(first, NEG, 0.0)
        peaks = {}
        for step in range(blocks + 2):
            ahead, here, behind = step, step - 1, step - 2
            peaks[ahead] = []
            if 0 <= here < blocks:
                peak = functools.reduce(jnp.maximum, peaks[here])
                total = jnp.zeros((1, 2 * BLK), F32)
                delta = jnp.zeros((1, 2 * BLK), F32)
                clipped = jnp.zeros((1, 2 * BLK), F32)
            for j in range(5):
                if ahead < blocks:
                    score(ahead, j, peaks[ahead])
                if 0 <= here < blocks:
                    e = jnp.exp(s_s[here % 2, tile(j), :] - (peak - penalty if j < LEFT // 2 - here else peak))
                    s_s[here % 2, tile(j), :] = e
                    total = total + jnp.sum(e, axis=0, keepdims=True)
                    delta = delta + jnp.sum(e * dw_s[here % 2, tile(j), :], axis=0, keepdims=True)
            if 0 <= here < blocks:
                inverse = 1.0 / total
                delta = delta * inverse
            if behind >= 0:
                query_side(behind)
            for j in range(5):
                if behind >= 0:
                    product(behind, j)
                if 0 <= here < blocks:
                    w = s_s[here % 2, tile(j), :] * inverse
                    ds = w * (dw_s[here % 2, tile(j), :] - delta)
                    if j < 2:
                        clipped = clipped + jnp.sum(ds, axis=0, keepdims=True)
                    else:
                        acc_s[tile(j - 2), :] += ds
                    ds_s[here % 2, tile(j), :] = ds.astype(BF16)
                    w_s[here % 2, tile(j), :] = w.astype(BF16)
            if 0 <= here < blocks:
                clip_s[...] += clipped
        gk_s[...] += jnp.sum(dk_s[slot] * khat_s[...], axis=0, keepdims=True)
        ck_s[p] = dk_s[slot, :REACH, :].astype(BF16)
        cv_s[p] = dv_s[slot, :REACH, :].astype(BF16)
        @pl.when(jnp.logical_not(first))
        def _():
            for copy in cross_copies(p):
                copy.start()

        lane = lax.broadcasted_iota(jnp.int32, (1, 512), 1)
        rows = []
        for head in range(2):
            far = jnp.sum(clip_s[:, head * BLK : (head + 1) * BLK], axis=1, keepdims=True)
            row = fold_bias(acc_s, head) + jnp.where(lane == 0, far, 0.0)
            rows += [row[:, b * BLK : (b + 1) * BLK] for b in range(4)]
        bsum_s[0, p] = jnp.concatenate(rows, axis=0)
        for copy in bias_copies(p):
            copy.start()

        @pl.when(p >= LAG)
        def _():
            finish(p - LAG, 0)

        return 0

    lax.fori_loop(0, pairs, pair, 0)
    gsum_s[0] = jnp.zeros(gsum_s.shape[1:], F32)
    gsum_s[0, 0:1, :] = gq_s[...]
    gsum_s[0, 1:2, :] = gk_s[...]
    gain_start(0)
    for r in range(count):
        bias_add(r)
        if r + 1 < count:
            for copy in late_copies(r + 1):
                copy.start()
        gain_add(r)
        if r + 1 < count:
            gain_start(r + 1)
    lax.fori_loop(max(pairs - LAG, 0), pairs, finish, 0)
    for p in range(pairs):
        out_ref[p] = bsum_s[count, p]
    out_ref[pairs] = gsum_s[count]

    @pl.when(jnp.logical_not(last))
    def _():
        for p in range(pairs):
            for copy in prior_copies(p):
                copy.wait_send()

    @pl.when(jnp.logical_not(first))
    def _():
        for p in range(pairs):
            for copy in cross_copies(p):
                copy.wait_send()

    for r in range(count):
        for copy in [copy for p in range(pairs) for copy in bias_copies(p)] if r == 0 else late_copies(r):
            copy.wait_send()
        for copy in gain_copies(r):
            copy.wait_send()


def drain(
    qg_ref, kg_ref, vg_ref, stat_ref, qg_hbm, kg_hbm, vg_hbm, bias_hbm, gq_hbm, gk_hbm,
    wide_s, bias_s, gq_s, gk_s, sem,
):
    moves = [(qg_ref, qg_hbm), (kg_ref, kg_hbm), (vg_ref, vg_hbm), (gq_s, gq_hbm), (gk_s, gk_hbm), (bias_s, bias_hbm)]
    copies = [pltpu.make_async_copy(src, dst, sem.at[n]) for n, (src, dst) in enumerate(moves)]
    for copy in copies[:3]:
        copy.start()
    heads, span = bias_s.shape
    pairs = heads // 2
    for row, ref in enumerate((gq_s, gk_s)):
        both = stat_ref[pairs, row : row + 1, :]
        ref[...] = (both + pltpu.roll(both, 64, 1))[:, :64].reshape(64)
    copies[3].start()
    copies[4].start()
    wide_s[...] = jnp.zeros_like(wide_s)
    for head in range(heads):
        for b in range(4):
            row = head % 2 * 4 + b
            wide_s[head : head + 1, b * BLK : (b + 1) * BLK] = stat_ref[head // 2, row : row + 1, :]
    wide = wide_s[...]
    lane = lax.broadcasted_iota(jnp.int32, wide.shape, 1)
    far = jnp.sum(jnp.where(lane <= 128, wide, 0.0), axis=1, keepdims=True)
    folded = jnp.where(lane == span - 1, far, pltpu.roll(wide, 319, 1))
    bias_s[...] = folded[:heads, :span]
    copies[5].start()
    for copy in copies:
        copy.wait()


def body(query_rows, key_rows, value_rows, query_gain, key_gain, position_bias, output_grad):
    heads = position_bias.shape[0]
    pairs = heads // 2
    tokens = query_rows.shape[0]
    sp, tp = lax.axis_size("sp"), lax.axis_size("tp")
    count = len(rounds_of(sp))
    group = 4 * tp
    ext = tokens + REACH
    padded = (heads + 7) // 8 * 8
    vmem, hbm = pl.BlockSpec(memory_space=pltpu.VMEM), pl.BlockSpec(memory_space=pltpu.HBM)
    shape = jax.ShapeDtypeStruct
    grads = shape((tokens, heads * 64), BF16)
    sems = pltpu.SemaphoreType.DMA
    operands = (
        query_rows, key_rows, value_rows, output_grad,
        query_gain.reshape(1, 64), key_gain.reshape(1, 64), position_bias,
    )
    results = pl.pallas_call(
        functools.partial(kernel, sp, tp),
        in_specs=[hbm] * 7,
        out_specs=[vmem] * 4,
        out_shape=[grads, grads, grads, shape((pairs + 1, 8, BLK), F32)],
        scratch_shapes=[pltpu.VMEM((tokens, heads * 64), BF16)] * 4
        + [
            pltpu.VMEM((ext, BLK), F32),
            pltpu.VMEM((ext, BLK), BF16), pltpu.VMEM((BLK, ext), BF16), pltpu.VMEM((ext, BLK), BF16),
            pltpu.VMEM((BAND, 2 * BLK), F32), pltpu.VMEM((3 * BLK, 2 * BLK), F32),
            pltpu.VMEM((2, BAND, 2 * BLK), F32), pltpu.VMEM((2, BAND, 2 * BLK), F32),
            pltpu.VMEM((2, BAND, 2 * BLK), BF16), pltpu.VMEM((2, BAND, 2 * BLK), BF16),
            pltpu.VMEM((tokens // BLK, 2 * BLK, BLK), BF16), pltpu.VMEM((tokens // BLK, 2 * BLK, BLK), BF16),
            pltpu.VMEM((tokens, BLK), F32), pltpu.VMEM((tokens, BLK), F32),
            pltpu.VMEM((pairs, ext, BLK), F32), pltpu.VMEM((pairs, ext, BLK), F32),
            pltpu.VMEM((1, 2 * BLK), F32), pltpu.VMEM((1, BLK), F32), pltpu.VMEM((1, BLK), F32),
        ]
        + [pltpu.VMEM((pairs, REACH, BLK), BF16)] * 6
        + [
            pltpu.VMEM((count + 1, pairs, 8, BLK), F32), pltpu.VMEM((count, 3, pairs, 8, BLK), F32),
            pltpu.VMEM((count + 1, 8, BLK), F32), pltpu.VMEM((count, 3, 8, BLK), F32), pltpu.VMEM((group, 8, BLK), F32),
            pltpu.VMEM((1, 64), BF16), pltpu.VMEM((1, 64), BF16), pltpu.VMEM(position_bias.shape, BF16),
            pltpu.VMEM((padded, 512), F32), pltpu.VMEM((padded, 512), F32), pltpu.VMEM((8, BLK), F32),
            sems((2, pairs)), sems((2, pairs)), sems((2, pairs)), sems((2, pairs)),
            sems((count, 3, pairs)), sems((count, 3, pairs)), sems((count, group)), sems((count, group)),
            sems((4, pairs)), sems((3,)),
        ],
        compiler_params=pltpu.CompilerParams(collective_id=0, has_side_effects=True, vmem_limit_bytes=48 << 20),
        name="attend",
    )(*[pltpu.with_memory_space_constraint(x, pltpu.HBM) for x in operands])
    return pl.pallas_call(
        drain,
        in_specs=[vmem] * 4,
        out_specs=[hbm] * 6,
        out_shape=[grads, grads, grads, shape(position_bias.shape, F32), shape((64,), F32), shape((64,), F32)],
        scratch_shapes=[
            pltpu.VMEM((padded, 512), F32), pltpu.VMEM(position_bias.shape, F32),
            pltpu.VMEM((64,), F32), pltpu.VMEM((64,), F32), sems((6,)),
        ],
        compiler_params=pltpu.CompilerParams(vmem_limit_bytes=2 << 20),
        name="drain",
    )(*results)


def solution(mesh):
    placed = (P("sp", "tp"), P("sp", "tp"), P("sp", "tp"), P(), P(), P("tp", None), P("sp", "tp"))
    return jax.shard_map(
        body,
        mesh=mesh,
        in_specs=placed,
        out_specs=(P("sp", "tp"), P("sp", "tp"), P("sp", "tp"), P("tp", None), P(), P()),
        check_vma=False,
    )
```

```python
import functools

import jax
import jax.numpy as jnp
from jax import lax
from jax.experimental import pallas as pl
from jax.experimental.pallas import tpu as pltpu
from jax.sharding import PartitionSpec as P

SEG = 64
LEFT = 8
REACH = SEG * LEFT
RSPAN = 320
NORM_EPS = 1e-06
BLK = 2 * SEG
BAND = REACH + BLK
NEG = -1e30
LAG = 2
AHEAD = 2
PART = 32
EARLY = 2
F32 = jnp.float32
BF16 = jnp.bfloat16


def dot(a, b, dims):
    return lax.dot_general(a, b, (dims, ((), ())), preferred_element_type=F32)


def half_ones():
    row = lax.broadcasted_iota(jnp.int32, (2 * BLK, BLK), 0) // 64 % 2
    col = lax.broadcasted_iota(jnp.int32, (2 * BLK, BLK), 1) // 64
    return jnp.where(row == col, 1.0, 0.0).astype(BF16)


def head_mean(x, ones):
    high = x.astype(BF16)
    low = (x - high.astype(F32)).astype(BF16)
    return dot(jnp.concatenate([high, low], axis=1), ones, ((1,), (0,))) * (1.0 / 64.0)


def normed(rows, ones):
    wide = rows.astype(F32)
    scale = lax.rsqrt(head_mean(wide * wide, ones) + NORM_EPS)
    return wide * scale, scale


def norm_grad(d_unit, gain, hat, scale, ones):
    scaled = d_unit * gain
    return scale * (scaled - hat * head_mean(scaled * hat, ones))


def stack_halves(x):
    lane = lax.broadcasted_iota(jnp.int32, x.shape, 1)
    zero = jnp.zeros_like(x)
    return jnp.concatenate([jnp.where(lane < 64, x, zero), jnp.where(lane < 64, zero, x)], axis=0)


def build_bias(table_row, bias_ref, head):
    wide = jnp.broadcast_to(table_row, (8, 512))
    sub = lax.broadcasted_iota(jnp.int32, (8, 512), 0)
    for bit in (1, 2, 4):
        wide = jnp.where((sub & bit) != 0, pltpu.roll(wide, bit, 1), wide)
    half = 8
    while half < BLK:
        wide = jnp.concatenate([wide, pltpu.roll(wide, half, 1)], axis=0)
        half *= 2
    lanes = slice(head * BLK, (head + 1) * BLK)
    row = lax.broadcasted_iota(jnp.int32, (BLK, BLK), 0)
    col = lax.broadcasted_iota(jnp.int32, (BLK, BLK), 1)
    far = jnp.broadcast_to(table_row[:, 0:1], (BLK, BLK))
    bias_ref[0:BLK, lanes] = jnp.where((row < SEG) & (col >= SEG), NEG, far)
    bias_ref[BLK : 2 * BLK, lanes] = far
    for j in range(3):
        tile = wide[:, ((4 - j) % 4) * BLK : ((4 - j) % 4) * BLK + BLK]
        if j == 2:
            tile = jnp.where((row >= SEG) & (col < SEG), NEG, tile)
        bias_ref[(2 + j) * BLK : (3 + j) * BLK, lanes] = tile


def fold_bias(acc_ref, head):
    lanes = slice(head * BLK, (head + 1) * BLK)
    tiles = [acc_ref[j * BLK : (j + 1) * BLK, lanes] for j in range(3)]
    wide = jnp.concatenate([tiles[0], jnp.zeros_like(tiles[0]), tiles[2], tiles[1]], axis=1)
    half = BLK // 2
    while half >= 8:
        wide = wide[:half] + pltpu.roll(wide[half:], 512 - half, 1)
        half //= 2
    for half in (4, 2, 1):
        wide = wide + pltpu.roll(pltpu.roll(wide, 512 - half, 1), 8 - half, 0)
    return wide[0:1]


def grouped(x):
    return x.reshape(x.shape[0] // 8, 8, x.shape[1])


def rounds_of(size):
    rounds, stride = [], 1
    while stride < size:
        radix = 4 if size // stride % 4 == 0 else 2
        rounds.append((stride, radix))
        stride *= radix
    return rounds


def peer(index, stride, radix, step):
    digit = (index // stride) % radix
    return index + stride * ((digit + step) % radix - digit)


def ring_sum(parts):
    if len(parts) == 4:
        return (parts[0] + parts[2]) + (parts[1] + parts[3])
    return parts[0] + parts[1] if len(parts) == 2 else parts[0]


def kernel(
    sp, tp, q_hbm, k_hbm, v_hbm, g_hbm, qgain_hbm, kgain_hbm, table_hbm,
    qg_ref, kg_ref, vg_ref, out_ref,
    q_ref, k_ref, v_ref, g_ref,
    k_s, kt_s, qs_s, gs_s, khat_s, kscale_s, qhat_s, qscale_s, nhat_s, dq_s,
    bias_s, acc_s, clip_s, e_s, dw_s, peak_s, factor_s, delta_s, ds_s, w_s, gq_s, gk_s,
    nq_s, ng_s, cq_s, bq_s, mid_s, own_s, next_s, before_s, after_s,
    bsum_s, bgot_s, gsum_s, ggot_s, gfirst_s,
    qgain_s, kgain_s, raw_s, wide_s, table_s, gains_s,
    rows_send, rows_recv, back_send, back_recv, part_send, part_recv,
    bias_send, bias_recv, gain_send, gain_recv, load_sem, small_sem,
):
    tokens = q_ref.shape[0]
    blocks = tokens // BLK
    cross = REACH // BLK
    pairs = nq_s.shape[0]
    tiles = {}
    for qb in range(blocks + cross):
        for kb in range(max(qb - cross, 0), min(qb + 1, blocks)):
            tiles[qb, kb] = len(tiles)
    me = lax.axis_index("sp")
    me_tp = lax.axis_index("tp")
    right, left = lax.rem(me + 1, sp), lax.rem(me + sp - 1, sp)
    rounds = rounds_of(sp)
    count = len(rounds)
    peers = [[{"sp": peer(me, stride, radix, k)} for k in range(1, radix)] for stride, radix in rounds]
    combos = [(k, t) for k in range(rounds[0][1]) for t in range(tp) if k or t]
    nearby = [{"sp": peer(me, 1, rounds[0][1], k), "tp": lax.rem(me_tp + t, tp)} for k, t in combos]
    first, last = me == 0, me == sp - 1
    has_left, has_right = jnp.logical_not(first), jnp.logical_not(last)

    def tile(j):
        return slice(j * BLK, (j + 1) * BLK)

    def wide_tile(j):
        return slice(j * 2 * BLK, (j + 1) * 2 * BLK)

    def lanes_of(p):
        return pl.ds(pl.multiple_of(p * BLK, BLK), BLK)

    def loads(p):
        moves = ((k_hbm, k_ref), (q_hbm, q_ref), (v_hbm, v_ref), (g_hbm, g_ref))
        return [
            pltpu.make_async_copy(src.at[:, lanes_of(p)], dst.at[:, lanes_of(p)], load_sem.at[n, p])
            for n, (src, dst) in enumerate(moves)
        ]

    smalls = [
        pltpu.make_async_copy(src, dst, small_sem.at[n])
        for n, (src, dst) in enumerate(((qgain_hbm, qgain_s), (kgain_hbm, kgain_s), (table_hbm, raw_s)))
    ]
    for copy in smalls:
        copy.start()
    for p in range(pairs):
        for copy in loads(p):
            copy.start()

    barrier = pltpu.get_barrier_semaphore()
    greeted = [{"sp": right}, {"sp": left}] + nearby + [device for group in peers for device in group]
    for device in greeted:
        pl.semaphore_signal(barrier, inc=1, device_id=device, device_id_type=pl.DeviceIdType.MESH)
    pl.semaphore_wait(barrier, len(greeted))

    def remote(src, dst, send, recv, device):
        return pltpu.make_async_remote_copy(
            src_ref=src, dst_ref=dst, send_sem=send, recv_sem=recv,
            device_id=device, device_id_type=pl.DeviceIdType.MESH,
        )

    def row_copies(p):
        rows = slice(0, REACH)
        return (
            remote(q_hbm.at[rows, lanes_of(p)], nq_s.at[p], rows_send.at[0, p], rows_recv.at[0, p], {"sp": left}),
            remote(g_hbm.at[rows, lanes_of(p)], ng_s.at[p], rows_send.at[1, p], rows_recv.at[1, p], {"sp": left}),
        )

    def back_copy(p):
        return remote(cq_s.at[p], bq_s.at[p], back_send.at[p], back_recv.at[p], {"sp": right})

    def own_copy(p):
        return remote(own_s.at[p], after_s.at[p], part_send.at[0, p], part_recv.at[0, p], {"sp": left})

    def next_copy(p):
        return remote(next_s.at[p], before_s.at[p], part_send.at[1, p], part_recv.at[1, p], {"sp": right})

    @pl.when(has_left)
    def _():
        for p in range(min(AHEAD, pairs)):
            for copy in row_copies(p):
                copy.start()

    @pl.when(first)
    def _():
        bq_s[...] = jnp.zeros_like(bq_s)
        before_s[...] = jnp.zeros_like(before_s)
        for p in range(pairs):
            before_s[p, 0:cross, :] = jnp.full((cross, 2 * BLK), NEG, F32)

    @pl.when(last)
    def _():
        nq_s[...] = jnp.zeros_like(nq_s)
        ng_s[...] = jnp.zeros_like(ng_s)
        after_s[...] = jnp.zeros_like(after_s)
        for p in range(pairs):
            after_s[p, 0:cross, :] = jnp.full((cross, 2 * BLK), -NEG, F32)
            after_s[p, cross : 2 * cross, :] = jnp.ones((cross, 2 * BLK), F32)

    def bias_copies(p):
        return [
            remote(bsum_s.at[0, p], bgot_s.at[0, k, p], bias_send.at[0, k, p], bias_recv.at[0, k, p], device)
            for k, device in enumerate(peers[0])
        ]

    def late_copies(r):
        return [
            remote(bsum_s.at[r], bgot_s.at[r, k], bias_send.at[r, k, 0], bias_recv.at[r, k, 0], device)
            for k, device in enumerate(peers[r])
        ]

    def bias_add(r):
        for copy in [copy for p in range(pairs) for copy in bias_copies(p)] if r == 0 else late_copies(r):
            copy.wait_recv()
        bsum_s[r + 1] = ring_sum([bsum_s[r]] + [bgot_s[r, k] for k in range(len(peers[r]))])

    def gain_copies(r):
        if r == 0:
            return [
                remote(gsum_s.at[0], gfirst_s.at[n], gain_send.at[0, n], gain_recv.at[0, n], device)
                for n, device in enumerate(nearby)
            ]
        return [
            remote(gsum_s.at[r], ggot_s.at[r, k], gain_send.at[r, k], gain_recv.at[r, k], device)
            for k, device in enumerate(peers[r])
        ]

    def gain_start(r):
        for copy in gain_copies(r):
            copy.start()

    def gain_add(r):
        for copy in gain_copies(r):
            copy.wait_recv()
        if r == 0:
            parts = {combo: gfirst_s[n] for n, combo in enumerate(combos)}
            parts[0, 0] = gsum_s[0]
            gsum_s[1] = ring_sum([ring_sum([parts[k, t] for t in range(tp)]) for k in range(rounds[0][1])])
        else:
            gsum_s[r + 1] = ring_sum([gsum_s[r]] + [ggot_s[r, k] for k in range(len(peers[r]))])

    ones = half_ones()
    for copy in smalls:
        copy.wait()
    for half in range(2):
        gains_s[0:1, half * 64 : half * 64 + 64] = qgain_s[...].astype(F32)
        gains_s[1:2, half * 64 : half * 64 + 64] = kgain_s[...].astype(F32)
    gain_q = gains_s[0:1, :]
    gain_k = gains_s[1:2, :]
    heads, span = raw_s.shape
    wide_s[...] = jnp.zeros_like(wide_s)
    wide_s[0:heads, 0:span] = raw_s[...].astype(F32)
    wide = wide_s[...]
    place = lax.broadcasted_iota(jnp.int32, wide.shape, 1)
    moved = pltpu.roll(wide, 193, 1)
    table_s[...] = jnp.where(place <= 128, wide[:, span - 1 : span], jnp.where(place < 193, NEG, moved))
    gq_s[...] = jnp.zeros_like(gq_s)
    gk_s[...] = jnp.zeros_like(gk_s)

    def query_tile(slot, qb, raw, grad):
        hat, scale = normed(raw, ones)
        qs_s[slot, wide_tile(qb), :] = stack_halves((hat * gain_q).astype(BF16) * jnp.asarray(0.125, BF16))
        gs_s[slot, wide_tile(qb), :] = stack_halves(grad)
        return hat, scale

    def scores(p, slot, qb):
        peaks, sums, deltas = [], [], []
        for kb in range(max(qb - cross, 0), min(qb + 1, blocks)):
            place = tiles[qb, kb]
            j = kb - qb + cross
            s = dot(k_s[slot, tile(kb), :], qs_s[slot, wide_tile(qb), :], ((1,), (1,))) + bias_s[tile(j), :]
            s = grouped(s)
            peak = jnp.max(s, axis=0)
            e = jnp.exp(s - peak[None])
            dw = dot(v_ref[tile(kb), lanes_of(p)], gs_s[slot, wide_tile(qb), :], ((1,), (1,)))
            e_s[slot, place] = e.reshape(BLK, 2 * BLK)
            dw_s[slot, place] = dw
            peak_s[slot, place] = peak
            peaks.append(peak)
            sums.append(jnp.sum(e, axis=0))
            deltas.append(jnp.sum(e * grouped(dw), axis=0))
        peak = jnp.max(functools.reduce(jnp.maximum, peaks), axis=0, keepdims=True)
        total = jnp.zeros((8, 2 * BLK), F32)
        delta = jnp.zeros((8, 2 * BLK), F32)
        for part, a, b in zip(peaks, sums, deltas):
            factor = jnp.exp(part - peak)
            total = total + a * factor
            delta = delta + b * factor
        found = (peak, jnp.sum(total, axis=0, keepdims=True), jnp.sum(delta, axis=0, keepdims=True))
        for n, row in enumerate(found):
            if qb < cross:
                own_s[p, n * cross + qb : n * cross + qb + 1, :] = row
            elif qb < blocks:
                mid_s[slot, n : n + 1, :] = row
            else:
                at = n * cross + qb - blocks
                next_s[p, at : at + 1, :] = row

    def forward(p):
        slot = lax.rem(p, 2)
        for copy in loads(p):
            copy.wait()

        def prepare(b):
            hat, scale = normed(k_ref[tile(b), lanes_of(p)], ones)
            khat_s[slot, tile(b), :] = hat
            kscale_s[slot, tile(b), :] = scale
            unit = hat * gain_k
            k_s[slot, tile(b), :] = unit.astype(BF16)
            kt_s[lax.rem(p, 3), :, tile(b)] = unit.T.astype(BF16)
            hat, scale = query_tile(slot, b, q_ref[tile(b), lanes_of(p)], g_ref[tile(b), lanes_of(p)])
            qhat_s[p, tile(b), :] = hat
            qscale_s[p, tile(b), :] = scale

        past = jnp.maximum(p - 2, 0)
        for b in range(EARLY):
            prepare(b)
        for b in range(blocks):
            if b + EARLY < blocks:
                prepare(b + EARLY)
            rest_query(past, b, p >= 2)
            scores(p, slot, b)
        rest_bias(past)

        @pl.when(p >= 2)
        def _():
            for copy in bias_copies(past):
                copy.start()

        @pl.when(has_left)
        def _():
            own_copy(p).start()

        @pl.when(has_left & (p + AHEAD < pairs))
        def _():
            for copy in row_copies(p + AHEAD):
                copy.start()

        @pl.when(has_right)
        def _():
            for copy in row_copies(p):
                copy.wait_recv()

        for b in range(cross):
            hat, _ = query_tile(slot, blocks + b, nq_s[p, tile(b), :], ng_s[p, tile(b), :])
            nhat_s[slot, tile(b), :] = hat
        for b in range(cross):
            scores(p, slot, blocks + b)

        @pl.when(has_right)
        def _():
            next_copy(p).start()

    def next_bias(p):
        for head in range(2):
            build_bias(table_s[pl.ds(p * 2 + head, 1), :], bias_s, head)

    def settle(mine, other):
        here, there = mine[:cross], other[:cross]
        peak = jnp.maximum(here, there)
        a, b = jnp.exp(here - peak), jnp.exp(there - peak)
        total = mine[cross : 2 * cross] * a + other[cross : 2 * cross] * b
        delta = mine[2 * cross : 3 * cross] * a + other[2 * cross : 3 * cross] * b
        inverse = 1.0 / total
        return peak, inverse, delta * inverse

    def backward(p):
        slot = lax.rem(p, 2)

        @pl.when(has_left)
        def _():
            next_copy(p).wait_recv()

        @pl.when(has_right)
        def _():
            own_copy(p).wait_recv()

        own = settle(own_s[p], before_s[p])
        later = settle(next_s[p], after_s[p])
        inverse = 1.0 / mid_s[slot, 1:2, :]
        mid = (mid_s[slot, 0:1, :], inverse, mid_s[slot, 2:3, :] * inverse)
        for qb in range(blocks + cross):
            found, at = (own, qb) if qb < cross else (mid, 0) if qb < blocks else (later, qb - blocks)
            peak, inverse, delta = (x[at : at + 1] for x in found)
            delta_s[qb] = jnp.broadcast_to(delta, (8, 2 * BLK))
            for kb in range(max(qb - cross, 0), min(qb + 1, blocks)):
                place = tiles[qb, kb]
                factor_s[place] = jnp.exp(peak_s[slot, place] - peak) * inverse

        clipped = jnp.zeros((8, 2 * BLK), F32)
        gain_sum = jnp.zeros((1, BLK), F32)
        for kb in reversed(range(blocks)):
            for qb in range(kb, kb + cross + 1):
                place, j = tiles[qb, kb], kb - qb + cross
                for part in range(BLK // PART):
                    rows = slice(part * PART, (part + 1) * PART)
                    w = grouped(e_s[slot, place, rows, :]) * factor_s[place][None]
                    ds = w * (grouped(dw_s[slot, place, rows, :]) - delta_s[qb][None])
                    if j < 2:
                        clipped = clipped + jnp.sum(ds, axis=0)
                    ds, w = ds.reshape(PART, 2 * BLK), w.reshape(PART, 2 * BLK)
                    if j >= 2:
                        at = slice((j - 2) * BLK + part * PART, (j - 2) * BLK + (part + 1) * PART)
                        acc_s[at, :] = ds if kb == blocks - 1 else acc_s[at, :] + ds
                    at = slice(kb * BLK + part * PART, kb * BLK + (part + 1) * PART)
                    ds_s[at, wide_tile(qb)] = ds.astype(BF16)
                    w_s[at, wide_tile(qb)] = w.astype(BF16)
            inner = slice(kb * 2 * BLK, blocks * 2 * BLK)
            outer = slice(blocks * 2 * BLK, (kb + cross + 1) * 2 * BLK)
            dk = dot(ds_s[tile(kb), inner], qs_s[slot, inner, :], ((1,), (0,)))
            dv = dot(w_s[tile(kb), inner], gs_s[slot, inner, :], ((1,), (0,)))
            if kb + cross >= blocks:
                dk = dk + dot(ds_s[tile(kb), outer], qs_s[slot, outer, :], ((1,), (0,))).astype(BF16).astype(F32)
                dv = dv + dot(w_s[tile(kb), outer], gs_s[slot, outer, :], ((1,), (0,))).astype(BF16).astype(F32)
            hat = khat_s[slot, tile(kb), :]
            gain_sum = gain_sum + jnp.sum(dk * hat, axis=0, keepdims=True)
            kg_ref[tile(kb), lanes_of(p)] = norm_grad(dk, gain_k, hat, kscale_s[slot, tile(kb), :], ones).astype(BF16)
            vg_ref[tile(kb), lanes_of(p)] = dv.astype(BF16)
            if kb > 0:
                query_side(p, slot, kb + cross)
        gk_s[...] += gain_sum
        clip_s[...] = clipped
        next_bias(jnp.minimum(p + 2, pairs - 1))

        @pl.when(has_right)
        def _():
            back_copy(p).start()

    def turned(p, qb):
        keys = slice(max(qb - cross, 0) * BLK, min(qb + 1, blocks) * BLK)
        dqt = dot(kt_s[lax.rem(p, 3), :, keys], ds_s[keys, wide_tile(qb)], ((1,), (0,)))
        dqt = jnp.concatenate([dqt[:64, :BLK], dqt[64:, BLK:]], axis=0)
        return dqt.T * 0.125

    def query_side(p, slot, qb):
        dq = turned(p, qb)
        cq_s[p, tile(qb - blocks), :] = dq.astype(BF16)
        gq_s[...] += jnp.sum(dq * nhat_s[slot, tile(qb - blocks), :], axis=0, keepdims=True)

    def rest_query(p, qb, live):
        dq = turned(p, qb)
        dq_s[p, tile(qb), :] = dq
        part = jnp.sum(dq * qhat_s[p, tile(qb), :], axis=0, keepdims=True)
        gq_s[...] += jnp.where(live, part, 0.0)

    def rest_bias(p):
        lane = lax.broadcasted_iota(jnp.int32, (1, 512), 1)
        rows = []
        clipped = jnp.sum(clip_s[...], axis=0, keepdims=True)
        for head in range(2):
            far = jnp.sum(clipped[:, head * BLK : (head + 1) * BLK], axis=1, keepdims=True)
            row = fold_bias(acc_s, head) + jnp.where(lane == 0, far, 0.0)
            rows += [row[:, b * BLK : (b + 1) * BLK] for b in range(4)]
        bsum_s[0, p] = jnp.concatenate(rows, axis=0)

    def rest(p):
        for qb in range(blocks):
            rest_query(p, qb, True)
        rest_bias(p)
        for copy in bias_copies(p):
            copy.start()

    def finish(p, _):
        @pl.when(has_left)
        def _():
            back_copy(p).wait_recv()

        for b in range(blocks):
            dq = dq_s[p, tile(b), :]
            if b < cross:
                dq = dq + bq_s[p, tile(b), :].astype(F32)
            grad = norm_grad(dq, gain_q, qhat_s[p, tile(b), :], qscale_s[p, tile(b), :], ones)
            qg_ref[tile(b), lanes_of(p)] = grad.astype(BF16)

        @pl.when(has_left)
        def _():
            for copy in (*row_copies(p), own_copy(p)):
                copy.wait_send()

        @pl.when(has_right)
        def _():
            for copy in (back_copy(p), next_copy(p)):
                copy.wait_send()

        for copy in bias_copies(p):
            copy.wait_send()
        return 0

    def step(t, _):
        @pl.when(t < pairs)
        def _():
            forward(t)

        @pl.when(t == pairs)
        def _():
            rest(pairs - 2)

        @pl.when(t == 0)
        def _():
            next_bias(min(1, pairs - 1))

        @pl.when(t >= 1)
        def _():
            backward(t - 1)

        @pl.when(t >= 1 + LAG)
        def _():
            finish(t - 1 - LAG, 0)

        return 0

    next_bias(0)
    lax.fori_loop(0, pairs + 1, step, 0)
    rest(pairs - 1)
    gsum_s[0] = jnp.zeros(gsum_s.shape[1:], F32)
    gsum_s[0, 0:1, :] = gq_s[...]
    gsum_s[0, 1:2, :] = gk_s[...]
    gain_start(0)
    for r in range(count):
        bias_add(r)
        if r + 1 < count:
            for copy in late_copies(r + 1):
                copy.start()
        gain_add(r)
        if r + 1 < count:
            gain_start(r + 1)
    lax.fori_loop(max(pairs - LAG, 0), pairs, finish, 0)
    for p in range(pairs):
        out_ref[p] = bsum_s[count, p]
    out_ref[pairs] = gsum_s[count]

    for r in range(count):
        if r > 0:
            for copy in late_copies(r):
                copy.wait_send()
        for copy in gain_copies(r):
            copy.wait_send()


def drain(
    qg_ref, kg_ref, vg_ref, stat_ref, qg_hbm, kg_hbm, vg_hbm, bias_hbm, gq_hbm, gk_hbm,
    wide_s, bias_s, gq_s, gk_s, sem,
):
    moves = [(qg_ref, qg_hbm), (kg_ref, kg_hbm), (vg_ref, vg_hbm), (gq_s, gq_hbm), (gk_s, gk_hbm), (bias_s, bias_hbm)]
    copies = [pltpu.make_async_copy(src, dst, sem.at[n]) for n, (src, dst) in enumerate(moves)]
    for copy in copies[:3]:
        copy.start()
    heads, span = bias_s.shape
    pairs = heads // 2
    for row, ref in enumerate((gq_s, gk_s)):
        both = stat_ref[pairs, row : row + 1, :]
        ref[...] = (both + pltpu.roll(both, 64, 1))[:, :64].reshape(64)
    copies[3].start()
    copies[4].start()
    wide_s[...] = jnp.zeros_like(wide_s)
    for head in range(heads):
        for b in range(4):
            row = head % 2 * 4 + b
            wide_s[head : head + 1, b * BLK : (b + 1) * BLK] = stat_ref[head // 2, row : row + 1, :]
    wide = wide_s[...]
    lane = lax.broadcasted_iota(jnp.int32, wide.shape, 1)
    far = jnp.sum(jnp.where(lane <= 128, wide, 0.0), axis=1, keepdims=True)
    folded = jnp.where(lane == span - 1, far, pltpu.roll(wide, 319, 1))
    bias_s[...] = folded[:heads, :span]
    copies[5].start()
    for copy in copies:
        copy.wait()


def body(query_rows, key_rows, value_rows, query_gain, key_gain, position_bias, output_grad):
    heads = position_bias.shape[0]
    pairs = heads // 2
    tokens = query_rows.shape[0]
    sp, tp = lax.axis_size("sp"), lax.axis_size("tp")
    count = len(rounds_of(sp))
    group = 4 * tp
    ext = tokens + REACH
    held = (REACH // BLK + 1) * (tokens // BLK)
    padded = (heads + 7) // 8 * 8
    vmem, hbm = pl.BlockSpec(memory_space=pltpu.VMEM), pl.BlockSpec(memory_space=pltpu.HBM)
    shape = jax.ShapeDtypeStruct
    grads = shape((tokens, heads * 64), BF16)
    sems = pltpu.SemaphoreType.DMA
    operands = (
        query_rows, key_rows, value_rows, output_grad,
        query_gain.reshape(1, 64), key_gain.reshape(1, 64), position_bias,
    )
    results = pl.pallas_call(
        functools.partial(kernel, sp, tp),
        in_specs=[hbm] * 7,
        out_specs=[vmem] * 4,
        out_shape=[grads, grads, grads, shape((pairs + 1, 8, BLK), F32)],
        scratch_shapes=[pltpu.VMEM((tokens, heads * 64), BF16)] * 4
        + [
            pltpu.VMEM((2, tokens, BLK), BF16), pltpu.VMEM((3, BLK, tokens), BF16),
            pltpu.VMEM((2, ext * 2, BLK), BF16), pltpu.VMEM((2, ext * 2, BLK), BF16),
            pltpu.VMEM((2, tokens, BLK), F32), pltpu.VMEM((2, tokens, BLK), F32),
            pltpu.VMEM((pairs, tokens, BLK), F32), pltpu.VMEM((pairs, tokens, BLK), F32),
            pltpu.VMEM((2, REACH, BLK), F32), pltpu.VMEM((pairs, tokens, BLK), F32),
            pltpu.VMEM((BAND, 2 * BLK), F32), pltpu.VMEM((3 * BLK, 2 * BLK), F32), pltpu.VMEM((8, 2 * BLK), F32),
            pltpu.VMEM((2, held, BLK, 2 * BLK), F32), pltpu.VMEM((2, held, BLK, 2 * BLK), F32),
            pltpu.VMEM((2, held, 8, 2 * BLK), F32), pltpu.VMEM((held, 8, 2 * BLK), F32),
            pltpu.VMEM((ext // BLK, 8, 2 * BLK), F32),
            pltpu.VMEM((tokens, ext * 2), BF16), pltpu.VMEM((tokens, ext * 2), BF16),
            pltpu.VMEM((1, BLK), F32), pltpu.VMEM((1, BLK), F32),
        ]
        + [pltpu.VMEM((pairs, REACH, BLK), BF16)] * 4
        + [pltpu.VMEM((2, 8, 2 * BLK), F32)]
        + [pltpu.VMEM((pairs, 16, 2 * BLK), F32)] * 4
        + [
            pltpu.VMEM((count + 1, pairs, 8, BLK), F32), pltpu.VMEM((count, 3, pairs, 8, BLK), F32),
            pltpu.VMEM((count + 1, 8, BLK), F32), pltpu.VMEM((count, 3, 8, BLK), F32), pltpu.VMEM((group, 8, BLK), F32),
            pltpu.VMEM((1, 64), BF16), pltpu.VMEM((1, 64), BF16), pltpu.VMEM(position_bias.shape, BF16),
            pltpu.VMEM((padded, 512), F32), pltpu.VMEM((padded, 512), F32), pltpu.VMEM((8, BLK), F32),
            sems((2, pairs)), sems((2, pairs)), sems((pairs,)), sems((pairs,)), sems((2, pairs)), sems((2, pairs)),
            sems((count, 3, pairs)), sems((count, 3, pairs)), sems((count, group)), sems((count, group)),
            sems((4, pairs)), sems((3,)),
        ],
        compiler_params=pltpu.CompilerParams(collective_id=0, has_side_effects=True, vmem_limit_bytes=48 << 20),
        name="attend",
    )(*[pltpu.with_memory_space_constraint(x, pltpu.HBM) for x in operands])
    return pl.pallas_call(
        drain,
        in_specs=[vmem] * 4,
        out_specs=[hbm] * 6,
        out_shape=[grads, grads, grads, shape(position_bias.shape, F32), shape((64,), F32), shape((64,), F32)],
        scratch_shapes=[
            pltpu.VMEM((padded, 512), F32), pltpu.VMEM(position_bias.shape, F32),
            pltpu.VMEM((64,), F32), pltpu.VMEM((64,), F32), sems((6,)),
        ],
        compiler_params=pltpu.CompilerParams(vmem_limit_bytes=2 << 20),
        name="drain",
    )(*results)


def solution(mesh):
    placed = (P("sp", "tp"), P("sp", "tp"), P("sp", "tp"), P(), P(), P("tp", None), P("sp", "tp"))
    return jax.shard_map(
        body,
        mesh=mesh,
        in_specs=placed,
        out_specs=(P("sp", "tp"), P("sp", "tp"), P("sp", "tp"), P("tp", None), P(), P()),
        check_vma=False,
    )
```

```python
import functools

import jax
import jax.numpy as jnp
from jax import lax
from jax.experimental import pallas as pl
from jax.experimental.pallas import tpu as pltpu
from jax.sharding import PartitionSpec as P

SEG = 64
LEFT = 8
REACH = SEG * LEFT
RSPAN = 320
NORM_EPS = 1e-06
BLK = 2 * SEG
BAND = REACH + BLK
NEG = -1e30
SLOTS = 4
BIASES = 3
PLANE = 4
PART = 32
EARLY = 2
F32 = jnp.float32
BF16 = jnp.bfloat16


def dot(a, b, dims):
    return lax.dot_general(a, b, (dims, ((), ())), preferred_element_type=F32)


def half_ones():
    row = lax.broadcasted_iota(jnp.int32, (2 * BLK, BLK), 0) // 64 % 2
    col = lax.broadcasted_iota(jnp.int32, (2 * BLK, BLK), 1) // 64
    return jnp.where(row == col, 1.0, 0.0).astype(BF16)


def head_mean(x, ones):
    high = x.astype(BF16)
    low = (x - high.astype(F32)).astype(BF16)
    return dot(jnp.concatenate([high, low], axis=1), ones, ((1,), (0,))) * (1.0 / 64.0)


def normed(rows, ones):
    wide = rows.astype(F32)
    scale = lax.rsqrt(head_mean(wide * wide, ones) + NORM_EPS)
    return wide * scale, scale


def norm_grad(d_unit, gain, hat, scale, ones):
    scaled = d_unit * gain
    return scale * (scaled - hat * head_mean(scaled * hat, ones))


def stack_halves(x):
    lane = lax.broadcasted_iota(jnp.int32, x.shape, 1)
    zero = jnp.zeros_like(x)
    return jnp.concatenate([jnp.where(lane < 64, x, zero), jnp.where(lane < 64, zero, x)], axis=0)


def build_bias(table_row, bias_ref, head):
    wide = jnp.broadcast_to(table_row, (8, 512))
    sub = lax.broadcasted_iota(jnp.int32, (8, 512), 0)
    for bit in (1, 2, 4):
        wide = jnp.where((sub & bit) != 0, pltpu.roll(wide, bit, 1), wide)
    half = 8
    while half < BLK:
        wide = jnp.concatenate([wide, pltpu.roll(wide, half, 1)], axis=0)
        half *= 2
    lanes = slice(head * BLK, (head + 1) * BLK)
    row = lax.broadcasted_iota(jnp.int32, (BLK, BLK), 0)
    col = lax.broadcasted_iota(jnp.int32, (BLK, BLK), 1)
    far = jnp.broadcast_to(table_row[:, 0:1], (BLK, BLK))
    bias_ref[0:BLK, lanes] = jnp.where((row < SEG) & (col >= SEG), NEG, far)
    bias_ref[BLK : 2 * BLK, lanes] = far
    for j in range(3):
        tile = wide[:, ((4 - j) % 4) * BLK : ((4 - j) % 4) * BLK + BLK]
        if j == 2:
            tile = jnp.where((row >= SEG) & (col < SEG), NEG, tile)
        bias_ref[(2 + j) * BLK : (3 + j) * BLK, lanes] = tile


def fold_bias(acc_ref, head):
    lanes = slice(head * BLK, (head + 1) * BLK)
    tiles = [acc_ref[j * BLK : (j + 1) * BLK, lanes] for j in range(3)]
    wide = jnp.concatenate([tiles[0], jnp.zeros_like(tiles[0]), tiles[2], tiles[1]], axis=1)
    half = BLK // 2
    while half >= 8:
        wide = wide[:half] + pltpu.roll(wide[half:], 512 - half, 1)
        half //= 2
    for half in (4, 2, 1):
        wide = wide + pltpu.roll(pltpu.roll(wide, 512 - half, 1), 8 - half, 0)
    return wide[0:1]


def grouped(x):
    return x.reshape(x.shape[0] // 8, 8, x.shape[1])


def rounds_of(size):
    rounds, stride = [], 1
    while stride < size:
        radix = 4 if size // stride % 4 == 0 else 2
        rounds.append((stride, radix))
        stride *= radix
    return rounds


def peer(index, stride, radix, step):
    digit = (index // stride) % radix
    return index + stride * ((digit + step) % radix - digit)


def ring_sum(parts):
    if len(parts) == 4:
        return (parts[0] + parts[2]) + (parts[1] + parts[3])
    return parts[0] + parts[1] if len(parts) == 2 else parts[0]


def kernel(
    sp, tp, q_hbm, k_hbm, v_hbm, g_hbm, qgain_hbm, kgain_hbm, table_hbm,
    qg_ref, kg_ref, vg_ref, out_ref,
    v_ref, k_s, kt_s, qs_s, gs_s, kscale_s, qscale_s, nhat_s, dq_s,
    bias_s, acc_s, clip_s, e_s, dw_s, later_e_s, later_dw_s, peak_s, factor_s, delta_s, ds_s, w_s, gq_s, gk_s,
    nq_s, ng_s, cq_s, bq_s, mid_s, own_s, next_s, before_s, after_s,
    bsum_s, bgot_s, gsum_s, ggot_s, gfirst_s,
    qgain_s, kgain_s, raw_s, wide_s, table_s, gains_s,
    rows_send, rows_recv, back_send, back_recv, part_send, part_recv,
    bias_send, bias_recv, gain_send, gain_recv, load_sem, small_sem,
):
    q_ref, k_ref, g_ref = qg_ref, kg_ref, vg_ref
    tokens = v_ref.shape[0]
    blocks = tokens // BLK
    cross = REACH // BLK
    pairs = nq_s.shape[0]
    tiles, own_tiles = {}, 0
    for qb in range(blocks + cross):
        if qb == blocks:
            own_tiles = len(tiles)
        for kb in range(max(qb - cross, 0), min(qb + 1, blocks)):
            tiles[qb, kb] = len(tiles)
    me = lax.axis_index("sp")
    me_tp = lax.axis_index("tp")
    right, left = lax.rem(me + 1, sp), lax.rem(me + sp - 1, sp)
    rounds = rounds_of(sp)
    count = len(rounds)
    peers = [[{"sp": peer(me, stride, radix, k)} for k in range(1, radix)] for stride, radix in rounds]
    combos = [(k, t) for k in range(rounds[0][1]) for t in range(tp) if k or t]
    nearby = [{"sp": peer(me, 1, rounds[0][1], k), "tp": lax.rem(me_tp + t, tp)} for k, t in combos]
    first, last = me == 0, me == sp - 1
    far = lax.rem(me, PLANE) == 0
    near_by = jnp.logical_not(far)
    has_left, has_right = jnp.logical_not(first), jnp.logical_not(last)

    def tile(j):
        return slice(j * BLK, (j + 1) * BLK)

    def wide_tile(j):
        return slice(j * 2 * BLK, (j + 1) * 2 * BLK)

    def held_at(p, place):
        if place < own_tiles:
            return e_s, dw_s, lax.rem(p, SLOTS), place
        return later_e_s, later_dw_s, lax.rem(p, SLOTS - 1), place - own_tiles

    def lanes_of(p):
        return pl.ds(pl.multiple_of(p * BLK, BLK), BLK)

    def loads(p):
        moves = ((k_hbm, k_ref), (q_hbm, q_ref), (v_hbm, v_ref), (g_hbm, g_ref))
        return [
            pltpu.make_async_copy(src.at[:, lanes_of(p)], dst.at[:, lanes_of(p)], load_sem.at[n, p])
            for n, (src, dst) in enumerate(moves)
        ]

    smalls = [
        pltpu.make_async_copy(src, dst, small_sem.at[n])
        for n, (src, dst) in enumerate(((qgain_hbm, qgain_s), (kgain_hbm, kgain_s), (table_hbm, raw_s)))
    ]
    for copy in smalls:
        copy.start()
    for p in range(pairs):
        for copy in loads(p):
            copy.start()

    barrier = pltpu.get_barrier_semaphore()
    greeted = [{"sp": right}, {"sp": left}] + nearby + [device for group in peers for device in group]
    for device in greeted:
        pl.semaphore_signal(barrier, inc=1, device_id=device, device_id_type=pl.DeviceIdType.MESH)
    ones = half_ones()
    for copy in smalls:
        copy.wait()
    for half in range(2):
        gains_s[0:1, half * 64 : half * 64 + 64] = qgain_s[...].astype(F32)
        gains_s[1:2, half * 64 : half * 64 + 64] = kgain_s[...].astype(F32)
    gain_q = gains_s[0:1, :]
    gain_k = gains_s[1:2, :]
    heads, span = raw_s.shape
    wide_s[...] = jnp.zeros_like(wide_s)
    wide_s[0:heads, 0:span] = raw_s[...].astype(F32)
    wide = wide_s[...]
    place = lax.broadcasted_iota(jnp.int32, wide.shape, 1)
    moved = pltpu.roll(wide, 193, 1)
    table_s[...] = jnp.where(place <= 128, wide[:, span - 1 : span], jnp.where(place < 193, NEG, moved))

    def next_bias(p):
        for head in range(2):
            build_bias(table_s[pl.ds(p * 2 + head, 1), :], bias_s.at[lax.rem(p, BIASES)], head)

    for p in range(min(2, pairs)):
        next_bias(p)
    pl.semaphore_wait(barrier, len(greeted))

    def remote(src, dst, send, recv, device):
        return pltpu.make_async_remote_copy(
            src_ref=src, dst_ref=dst, send_sem=send, recv_sem=recv,
            device_id=device, device_id_type=pl.DeviceIdType.MESH,
        )

    def row_copies(p):
        rows = slice(0, REACH)
        return (
            remote(q_hbm.at[rows, lanes_of(p)], nq_s.at[p], rows_send.at[0, p], rows_recv.at[0, p], {"sp": left}),
            remote(g_hbm.at[rows, lanes_of(p)], ng_s.at[p], rows_send.at[1, p], rows_recv.at[1, p], {"sp": left}),
        )

    def back_copy(p):
        return remote(cq_s.at[p], bq_s.at[p], back_send.at[p], back_recv.at[p], {"sp": right})

    def own_copy(p):
        return remote(own_s.at[p], after_s.at[p], part_send.at[0, p], part_recv.at[0, p], {"sp": left})

    def next_copy(p):
        return remote(next_s.at[p], before_s.at[p], part_send.at[1, p], part_recv.at[1, p], {"sp": right})

    @pl.when(has_left)
    def _():
        for copy in row_copies(0):
            copy.start()

    @pl.when(has_left)
    def _():
        for copy in row_copies(1):
            copy.start()

    @pl.when(first)
    def _():
        bq_s[...] = jnp.zeros_like(bq_s)
        before_s[...] = jnp.zeros_like(before_s)
        for p in range(pairs):
            before_s[p, 0:cross, :] = jnp.full((cross, 2 * BLK), NEG, F32)

    @pl.when(last)
    def _():
        nq_s[...] = jnp.zeros_like(nq_s)
        ng_s[...] = jnp.zeros_like(ng_s)
        after_s[...] = jnp.zeros_like(after_s)
        for p in range(pairs):
            after_s[p, 0:cross, :] = jnp.full((cross, 2 * BLK), -NEG, F32)
            after_s[p, cross : 2 * cross, :] = jnp.ones((cross, 2 * BLK), F32)

    early = pairs - 1

    def bias_copies(p):
        return [
            remote(bsum_s.at[0, p], bgot_s.at[0, k, p], bias_send.at[0, k, p], bias_recv.at[0, k, p], device)
            for k, device in enumerate(peers[0])
        ]

    def late_copies(r):
        return [
            remote(bsum_s.at[r], bgot_s.at[r, k], bias_send.at[r, k, 0], bias_recv.at[r, k, 0], device)
            for k, device in enumerate(peers[r])
        ]

    def bias_add(r):
        for copy in [copy for p in range(early) for copy in bias_copies(p)] if r == 0 else late_copies(r):
            copy.wait_recv()
        bsum_s[r + 1] = ring_sum([bsum_s[r]] + [bgot_s[r, k] for k in range(len(peers[r]))])
        if r + 1 < count:
            for copy in late_copies(r + 1):
                copy.start()

    def gain_copies(r):
        if r == 0:
            return [
                remote(gsum_s.at[0], gfirst_s.at[n], gain_send.at[0, n], gain_recv.at[0, n], device)
                for n, device in enumerate(nearby)
            ]
        return [
            remote(gsum_s.at[r], ggot_s.at[r, k], gain_send.at[r, k], gain_recv.at[r, k], device)
            for k, device in enumerate(peers[r])
        ]

    def gain_start(r):
        for copy in gain_copies(r):
            copy.start()

    def gain_add(r):
        for copy in gain_copies(r):
            copy.wait_recv()
        if r == 0:
            parts = {combo: gfirst_s[n] for n, combo in enumerate(combos)}
            parts[0, 0] = gsum_s[0]
            gsum_s[1, 0] = ring_sum([parts[k, 0][0] for k in range(rounds[0][1])])
            gsum_s[1, 1] = ring_sum([ring_sum([parts[k, t][1] for t in range(tp)]) for k in range(rounds[0][1])])
        else:
            gsum_s[r + 1] = ring_sum([gsum_s[r]] + [ggot_s[r, k] for k in range(len(peers[r]))])

    gq_s[...] = jnp.zeros_like(gq_s)
    gk_s[...] = jnp.zeros_like(gk_s)

    def query_tile(slot, qb, raw, grad):
        hat, scale = normed(raw, ones)
        qs_s[slot, wide_tile(qb), :] = stack_halves((hat * gain_q).astype(BF16) * jnp.asarray(0.125, BF16))
        gs_s[slot, wide_tile(qb), :] = stack_halves(grad)
        return hat, scale

    def scores(p, slot, qb):
        peaks, sums, deltas = [], [], []
        for kb in range(max(qb - cross, 0), min(qb + 1, blocks)):
            place = tiles[qb, kb]
            j = kb - qb + cross
            s = dot(k_s[slot, tile(kb), :], qs_s[slot, wide_tile(qb), :], ((1,), (1,))) + bias_s[lax.rem(p, BIASES), tile(j), :]
            s = grouped(s)
            peak = jnp.max(s, axis=0)
            e = jnp.exp(s - peak[None])
            dw = dot(v_ref[tile(kb), lanes_of(p)], gs_s[slot, wide_tile(qb), :], ((1,), (1,)))
            e_ref, dw_ref, at, spot = held_at(p, place)
            e_ref[at, spot] = e.reshape(BLK, 2 * BLK)
            dw_ref[at, spot] = dw
            peak_s[slot, place] = peak
            peaks.append(peak)
            sums.append(jnp.sum(e, axis=0))
            deltas.append(jnp.sum(e * grouped(dw), axis=0))
        peak = jnp.max(functools.reduce(jnp.maximum, peaks), axis=0, keepdims=True)
        total = jnp.zeros((8, 2 * BLK), F32)
        delta = jnp.zeros((8, 2 * BLK), F32)
        for part, a, b in zip(peaks, sums, deltas):
            factor = jnp.exp(part - peak)
            total = total + a * factor
            delta = delta + b * factor
        found = (peak, jnp.sum(total, axis=0, keepdims=True), jnp.sum(delta, axis=0, keepdims=True))
        for n, row in enumerate(found):
            if qb < cross:
                own_s[p, n * cross + qb : n * cross + qb + 1, :] = row
            elif qb < blocks:
                mid_s[slot, n : n + 1, :] = row
            else:
                at = n * cross + qb - blocks
                next_s[p, at : at + 1, :] = row

    def inner(p):
        slot = lax.rem(p, SLOTS)
        for copy in loads(p):
            copy.wait()

        def prepare(b):
            hat, scale = normed(k_ref[tile(b), lanes_of(p)], ones)
            kscale_s[slot, tile(b), :] = scale
            unit = hat * gain_k
            k_s[slot, tile(b), :] = unit.astype(BF16)
            kt_s[lax.rem(p, SLOTS + 1), :, tile(b)] = unit.T.astype(BF16)
            _, scale = query_tile(slot, b, q_ref[tile(b), lanes_of(p)], g_ref[tile(b), lanes_of(p)])
            qscale_s[p, tile(b), :] = scale

        for b in range(EARLY):
            prepare(b)
        for b in range(blocks):
            if b + EARLY < blocks:
                prepare(b + EARLY)
            scores(p, slot, b)

        @pl.when(has_left)
        def _():
            own_copy(p).start()

        @pl.when(has_left & near_by & (p == 0))
        def _():
            for copy in row_copies(2):
                copy.start()

    def outer(p):
        slot = lax.rem(p, SLOTS)

        @pl.when(has_right)
        def _():
            for copy in row_copies(p):
                copy.wait_recv()

        for b in range(cross):
            hat, _ = query_tile(slot, blocks + b, nq_s[p, tile(b), :], ng_s[p, tile(b), :])
            nhat_s[slot, tile(b), :] = hat
        past = jnp.maximum(p - 3, 0)
        for b in range(cross):
            rest_query(past, b, p >= 3)
            scores(p, slot, blocks + b)
        for b in range(cross, blocks):
            rest_query(past, b, p >= 3)
        bsum_s[0, past] = rest_bias(past)
        next_bias(jnp.minimum(p + 2, pairs - 1))

        @pl.when(has_right)
        def _():
            next_copy(p).start()

    def settle(mine, other):
        here, there = mine[:cross], other[:cross]
        peak = jnp.maximum(here, there)
        a, b = jnp.exp(here - peak), jnp.exp(there - peak)
        total = mine[cross : 2 * cross] * a + other[cross : 2 * cross] * b
        delta = mine[2 * cross : 3 * cross] * a + other[2 * cross : 3 * cross] * b
        inverse = 1.0 / total
        return peak, inverse, delta * inverse

    def backward(p):
        slot = lax.rem(p, SLOTS)

        @pl.when(has_left)
        def _():
            next_copy(p).wait_recv()

        @pl.when(has_right)
        def _():
            own_copy(p).wait_recv()

        @pl.when(has_left & (p + 3 < pairs) & (p <= 1) & far)
        def _():
            for copy in row_copies(p + 3):
                copy.start()

        own = settle(own_s[p], before_s[p])
        later = settle(next_s[p], after_s[p])
        inverse = 1.0 / mid_s[slot, 1:2, :]
        mid = (mid_s[slot, 0:1, :], inverse, mid_s[slot, 2:3, :] * inverse)
        for qb in range(blocks + cross):
            found, at = (own, qb) if qb < cross else (mid, 0) if qb < blocks else (later, qb - blocks)
            peak, inverse, delta = (x[at : at + 1] for x in found)
            delta_s[qb] = jnp.broadcast_to(delta, (8, 2 * BLK))
            for kb in range(max(qb - cross, 0), min(qb + 1, blocks)):
                place = tiles[qb, kb]
                factor_s[place] = jnp.exp(peak_s[slot, place] - peak) * inverse

        clipped = jnp.zeros((8, 2 * BLK), F32)
        gain_sum = jnp.zeros((1, BLK), F32)
        for kb in reversed(range(blocks)):
            for qb in range(kb, kb + cross + 1):
                place, j = tiles[qb, kb], kb - qb + cross
                e_ref, dw_ref, held, spot = held_at(p, place)
                for part in range(BLK // PART):
                    rows = slice(part * PART, (part + 1) * PART)
                    w = grouped(e_ref[held, spot, rows, :]) * factor_s[place][None]
                    ds = w * (grouped(dw_ref[held, spot, rows, :]) - delta_s[qb][None])
                    if j < 2:
                        clipped = clipped + jnp.sum(ds, axis=0)
                    ds, w = ds.reshape(PART, 2 * BLK), w.reshape(PART, 2 * BLK)
                    if j >= 2:
                        at = slice((j - 2) * BLK + part * PART, (j - 2) * BLK + (part + 1) * PART)
                        acc_s[at, :] = ds if kb == blocks - 1 else acc_s[at, :] + ds
                    at = slice(kb * BLK + part * PART, kb * BLK + (part + 1) * PART)
                    ds_s[at, wide_tile(qb)] = ds.astype(BF16)
                    w_s[at, wide_tile(qb)] = w.astype(BF16)
            near = slice(kb * 2 * BLK, blocks * 2 * BLK)
            away = slice(blocks * 2 * BLK, (kb + cross + 1) * 2 * BLK)
            dk = dot(ds_s[tile(kb), near], qs_s[slot, near, :], ((1,), (0,)))
            dv = dot(w_s[tile(kb), near], gs_s[slot, near, :], ((1,), (0,)))
            if kb + cross >= blocks:
                dk = dk + dot(ds_s[tile(kb), away], qs_s[slot, away, :], ((1,), (0,))).astype(BF16).astype(F32)
                dv = dv + dot(w_s[tile(kb), away], gs_s[slot, away, :], ((1,), (0,))).astype(BF16).astype(F32)
            hat = k_ref[tile(kb), lanes_of(p)].astype(F32) * kscale_s[slot, tile(kb), :]
            gain_sum = gain_sum + jnp.sum(dk * hat, axis=0, keepdims=True)
            kg_ref[tile(kb), lanes_of(p)] = norm_grad(dk, gain_k, hat, kscale_s[slot, tile(kb), :], ones).astype(BF16)
            vg_ref[tile(kb), lanes_of(p)] = dv.astype(BF16)
            if kb > 0:
                query_side(p, slot, kb + cross)
        gk_s[...] += gain_sum
        clip_s[...] = clipped

        @pl.when(has_right)
        def _():
            back_copy(p).start()

    def turned(p, qb):
        keys = slice(max(qb - cross, 0) * BLK, min(qb + 1, blocks) * BLK)
        dqt = dot(kt_s[lax.rem(p, SLOTS + 1), :, keys], ds_s[keys, wide_tile(qb)], ((1,), (0,)))
        dqt = jnp.concatenate([dqt[:64, :BLK], dqt[64:, BLK:]], axis=0)
        return dqt.T * 0.125

    def query_side(p, slot, qb):
        dq = turned(p, qb)
        cq_s[p, tile(qb - blocks), :] = dq.astype(BF16)
        gq_s[...] += jnp.sum(dq * nhat_s[slot, tile(qb - blocks), :], axis=0, keepdims=True)

    def rest_query(p, qb, live):
        dq = turned(p, qb)
        dq_s[p, tile(qb), :] = dq
        hat = q_ref[tile(qb), lanes_of(p)].astype(F32) * qscale_s[p, tile(qb), :]
        part = jnp.sum(dq * hat, axis=0, keepdims=True)
        gq_s[...] += jnp.where(live, part, 0.0)

    def rest_bias(p):
        lane = lax.broadcasted_iota(jnp.int32, (1, 512), 1)
        rows = []
        clipped = jnp.sum(clip_s[...], axis=0, keepdims=True)
        for head in range(2):
            far = jnp.sum(clipped[:, head * BLK : (head + 1) * BLK], axis=1, keepdims=True)
            row = fold_bias(acc_s, head) + jnp.where(lane == 0, far, 0.0)
            rows += [row[:, b * BLK : (b + 1) * BLK] for b in range(4)]
        return jnp.concatenate(rows, axis=0)

    def finish(p, _):
        @pl.when(has_left)
        def _():
            back_copy(p).wait_recv()

        for b in range(blocks):
            dq = dq_s[p, tile(b), :]
            if b < cross:
                dq = dq + bq_s[p, tile(b), :].astype(F32)
            scale = qscale_s[p, tile(b), :]
            hat = q_ref[tile(b), lanes_of(p)].astype(F32) * scale
            grad = norm_grad(dq, gain_q, hat, scale, ones)
            qg_ref[tile(b), lanes_of(p)] = grad.astype(BF16)

        @pl.when(has_left)
        def _():
            for copy in (*row_copies(p), own_copy(p)):
                copy.wait_send()

        @pl.when(has_right)
        def _():
            for copy in (back_copy(p), next_copy(p)):
                copy.wait_send()

        return 0

    def step(t, _):
        @pl.when(t < pairs)
        def _():
            inner(t)

        @pl.when((t >= 1) & (t <= pairs))
        def _():
            outer(t - 1)

        @pl.when(has_left & (t < pairs) & (t == 2) & far)
        def _():
            for copy in row_copies(t):
                copy.start()

        @pl.when(has_left & (t + 2 < pairs) & (t >= 1) & near_by)
        def _():
            for copy in row_copies(t + 2):
                copy.start()

        @pl.when(t > pairs)
        def _():
            for qb in range(blocks):
                rest_query(t - 4, qb, True)
            bsum_s[0, t - 4] = rest_bias(t - 4)

        @pl.when(t >= 4)
        def _():
            for copy in bias_copies(t - 4):
                copy.start()

        @pl.when(t >= 3)
        def _():
            backward(t - 3)

        @pl.when(has_left & (t >= 4) & (t + 1 < pairs) & far)
        def _():
            for copy in row_copies(t + 1):
                copy.start()

        return 0

    lax.fori_loop(0, pairs + 3, step, 0)
    for qb in range(blocks):
        rest_query(pairs - 1, qb, True)
    gsum_s[0, 0] = rest_bias(pairs - 1)
    gsum_s[0, 1] = jnp.zeros(gsum_s.shape[2:], F32)
    gsum_s[0, 1, 0:1, :] = gq_s[...]
    gsum_s[0, 1, 1:2, :] = gk_s[...]
    gain_start(0)
    for r in range(count):
        bias_add(r)
        if r == 0:
            lax.fori_loop(0, pairs // 2, finish, 0)
        gain_add(r)
        if r + 1 < count:
            gain_start(r + 1)
        if r == 0:
            lax.fori_loop(pairs // 2, pairs, finish, 0)
    for p in range(early):
        out_ref[p] = bsum_s[count, p]
    out_ref[early] = gsum_s[count, 0]
    out_ref[pairs] = gsum_s[count, 1]
    for p in range(early):
        for copy in bias_copies(p):
            copy.wait_send()
    for r in range(count):
        if r > 0:
            for copy in late_copies(r):
                copy.wait_send()
        for copy in gain_copies(r):
            copy.wait_send()


def drain(
    qg_ref, kg_ref, vg_ref, stat_ref, qg_hbm, kg_hbm, vg_hbm, bias_hbm, gq_hbm, gk_hbm,
    wide_s, bias_s, gq_s, gk_s, sem,
):
    moves = [(qg_ref, qg_hbm), (kg_ref, kg_hbm), (vg_ref, vg_hbm), (gq_s, gq_hbm), (gk_s, gk_hbm), (bias_s, bias_hbm)]
    copies = [pltpu.make_async_copy(src, dst, sem.at[n]) for n, (src, dst) in enumerate(moves)]
    for copy in copies[:3]:
        copy.start()
    heads, span = bias_s.shape
    pairs = heads // 2
    for row, ref in enumerate((gq_s, gk_s)):
        both = stat_ref[pairs, row : row + 1, :]
        ref[...] = (both + pltpu.roll(both, 64, 1))[:, :64].reshape(64)
    copies[3].start()
    copies[4].start()
    wide_s[...] = jnp.zeros_like(wide_s)
    for head in range(heads):
        for b in range(4):
            row = head % 2 * 4 + b
            wide_s[head : head + 1, b * BLK : (b + 1) * BLK] = stat_ref[head // 2, row : row + 1, :]
    wide = wide_s[...]
    lane = lax.broadcasted_iota(jnp.int32, wide.shape, 1)
    far = jnp.sum(jnp.where(lane <= 128, wide, 0.0), axis=1, keepdims=True)
    folded = jnp.where(lane == span - 1, far, pltpu.roll(wide, 319, 1))
    bias_s[...] = folded[:heads, :span]
    copies[5].start()
    for copy in copies:
        copy.wait()


def body(query_rows, key_rows, value_rows, query_gain, key_gain, position_bias, output_grad):
    heads = position_bias.shape[0]
    pairs = heads // 2
    tokens = query_rows.shape[0]
    sp, tp = lax.axis_size("sp"), lax.axis_size("tp")
    count = len(rounds_of(sp))
    group = 4 * tp
    ext = tokens + REACH
    reach, blocks = REACH // BLK, tokens // BLK
    held = (reach + 1) * blocks
    own = sum(min(qb, reach) + 1 for qb in range(blocks))
    padded = (heads + 7) // 8 * 8
    vmem, hbm = pl.BlockSpec(memory_space=pltpu.VMEM), pl.BlockSpec(memory_space=pltpu.HBM)
    shape = jax.ShapeDtypeStruct
    grads = shape((tokens, heads * 64), BF16)
    sems = pltpu.SemaphoreType.DMA
    operands = (
        query_rows, key_rows, value_rows, output_grad,
        query_gain.reshape(1, 64), key_gain.reshape(1, 64), position_bias,
    )
    results = pl.pallas_call(
        functools.partial(kernel, sp, tp),
        in_specs=[hbm] * 7,
        out_specs=[vmem] * 4,
        out_shape=[grads, grads, grads, shape((pairs + 1, 8, BLK), F32)],
        scratch_shapes=[pltpu.VMEM((tokens, heads * 64), BF16)]
        + [
            pltpu.VMEM((SLOTS, tokens, BLK), BF16), pltpu.VMEM((SLOTS + 1, BLK, tokens), BF16),
            pltpu.VMEM((SLOTS, ext * 2, BLK), BF16), pltpu.VMEM((SLOTS, ext * 2, BLK), BF16),
            pltpu.VMEM((SLOTS, tokens, BLK), F32), pltpu.VMEM((pairs, tokens, BLK), F32),
            pltpu.VMEM((SLOTS, REACH, BLK), F32), pltpu.VMEM((pairs, tokens, BLK), F32),
            pltpu.VMEM((BIASES, BAND, 2 * BLK), F32), pltpu.VMEM((3 * BLK, 2 * BLK), F32), pltpu.VMEM((8, 2 * BLK), F32),
            *[pltpu.VMEM((SLOTS, own, BLK, 2 * BLK), F32)] * 2, *[pltpu.VMEM((SLOTS - 1, held - own, BLK, 2 * BLK), F32)] * 2,
            pltpu.VMEM((SLOTS, held, 8, 2 * BLK), F32), pltpu.VMEM((held, 8, 2 * BLK), F32),
            pltpu.VMEM((ext // BLK, 8, 2 * BLK), F32),
            pltpu.VMEM((tokens, ext * 2), BF16), pltpu.VMEM((tokens, ext * 2), BF16),
            pltpu.VMEM((1, BLK), F32), pltpu.VMEM((1, BLK), F32),
        ]
        + [pltpu.VMEM((pairs, REACH, BLK), BF16)] * 4
        + [pltpu.VMEM((SLOTS, 8, 2 * BLK), F32)]
        + [pltpu.VMEM((pairs, 16, 2 * BLK), F32)] * 4
        + [
            pltpu.VMEM((count + 1, pairs - 1, 8, BLK), F32), pltpu.VMEM((count, 3, pairs - 1, 8, BLK), F32),
            pltpu.VMEM((count + 1, 2, 8, BLK), F32), pltpu.VMEM((count, 3, 2, 8, BLK), F32), pltpu.VMEM((group, 2, 8, BLK), F32),
            pltpu.VMEM((1, 64), BF16), pltpu.VMEM((1, 64), BF16), pltpu.VMEM(position_bias.shape, BF16),
            pltpu.VMEM((padded, 512), F32), pltpu.VMEM((padded, 512), F32), pltpu.VMEM((8, BLK), F32),
            sems((2, pairs)), sems((2, pairs)), sems((pairs,)), sems((pairs,)), sems((2, pairs)), sems((2, pairs)),
            sems((count, 3, pairs)), sems((count, 3, pairs)), sems((count, group)), sems((count, group)),
            sems((4, pairs)), sems((3,)),
        ],
        compiler_params=pltpu.CompilerParams(collective_id=0, has_side_effects=True, vmem_limit_bytes=50 << 20),
        name="attend",
    )(*[pltpu.with_memory_space_constraint(x, pltpu.HBM) for x in operands])
    return pl.pallas_call(
        drain,
        in_specs=[vmem] * 4,
        out_specs=[hbm] * 6,
        out_shape=[grads, grads, grads, shape(position_bias.shape, F32), shape((64,), F32), shape((64,), F32)],
        scratch_shapes=[
            pltpu.VMEM((padded, 512), F32), pltpu.VMEM(position_bias.shape, F32),
            pltpu.VMEM((64,), F32), pltpu.VMEM((64,), F32), sems((6,)),
        ],
        compiler_params=pltpu.CompilerParams(vmem_limit_bytes=2 << 20),
        name="drain",
    )(*results)


def solution(mesh):
    placed = (P("sp", "tp"), P("sp", "tp"), P("sp", "tp"), P(), P(), P("tp", None), P("sp", "tp"))
    return jax.shard_map(
        body,
        mesh=mesh,
        in_specs=placed,
        out_specs=(P("sp", "tp"), P("sp", "tp"), P("sp", "tp"), P("tp", None), P(), P()),
        check_vma=False,
    )
```

```python
import functools

import jax
import jax.numpy as jnp
from jax import lax
from jax.experimental import pallas as pl
from jax.experimental.pallas import tpu as pltpu
from jax.sharding import PartitionSpec as P

SEG = 64
LEFT = 8
REACH = SEG * LEFT
RSPAN = 320
NORM_EPS = 1e-06
BLK = 2 * SEG
BAND = REACH + BLK
NEG = -1e30
SLOTS = 4
BIASES = 3
PLANE = 4
PART = 16
EARLY = 2
F32 = jnp.float32
BF16 = jnp.bfloat16


def dot(a, b, dims):
    return lax.dot_general(a, b, (dims, ((), ())), preferred_element_type=F32)


def half_ones():
    row = lax.broadcasted_iota(jnp.int32, (2 * BLK, BLK), 0) // 64 % 2
    col = lax.broadcasted_iota(jnp.int32, (2 * BLK, BLK), 1) // 64
    return jnp.where(row == col, 1.0, 0.0).astype(BF16)


def head_mean(x, ones):
    high = x.astype(BF16)
    low = (x - high.astype(F32)).astype(BF16)
    return dot(jnp.concatenate([high, low], axis=1), ones, ((1,), (0,))) * (1.0 / 64.0)


def normed(rows, ones):
    wide = rows.astype(F32)
    scale = lax.rsqrt(head_mean(wide * wide, ones) + NORM_EPS)
    return wide * scale, scale


def norm_grad(d_unit, gain, hat, scale, ones):
    scaled = d_unit * gain
    return scale * (scaled - hat * head_mean(scaled * hat, ones))


def stack_halves(x):
    lane = lax.broadcasted_iota(jnp.int32, x.shape, 1)
    zero = jnp.zeros_like(x)
    return jnp.concatenate([jnp.where(lane < 64, x, zero), jnp.where(lane < 64, zero, x)], axis=0)


def build_bias(table_row, bias_ref, head):
    wide = jnp.broadcast_to(table_row, (8, 512))
    sub = lax.broadcasted_iota(jnp.int32, (8, 512), 0)
    for bit in (1, 2, 4):
        wide = jnp.where((sub & bit) != 0, pltpu.roll(wide, bit, 1), wide)
    half = 8
    while half < BLK:
        wide = jnp.concatenate([wide, pltpu.roll(wide, half, 1)], axis=0)
        half *= 2
    lanes = slice(head * BLK, (head + 1) * BLK)
    row = lax.broadcasted_iota(jnp.int32, (BLK, BLK), 0)
    col = lax.broadcasted_iota(jnp.int32, (BLK, BLK), 1)
    far = jnp.broadcast_to(table_row[:, 0:1], (BLK, BLK))
    bias_ref[0:BLK, lanes] = jnp.where((row < SEG) & (col >= SEG), NEG, far)
    bias_ref[BLK : 2 * BLK, lanes] = far
    for j in range(3):
        tile = wide[:, ((4 - j) % 4) * BLK : ((4 - j) % 4) * BLK + BLK]
        if j == 2:
            tile = jnp.where((row >= SEG) & (col < SEG), NEG, tile)
        bias_ref[(2 + j) * BLK : (3 + j) * BLK, lanes] = tile


def fold_bias(acc_ref, head):
    lanes = slice(head * BLK, (head + 1) * BLK)
    tiles = [acc_ref[j * BLK : (j + 1) * BLK, lanes] for j in range(3)]
    wide = jnp.concatenate([tiles[0], jnp.zeros_like(tiles[0]), tiles[2], tiles[1]], axis=1)
    half = BLK // 2
    while half >= 8:
        wide = wide[:half] + pltpu.roll(wide[half:], 512 - half, 1)
        half //= 2
    for half in (4, 2, 1):
        wide = wide + pltpu.roll(pltpu.roll(wide, 512 - half, 1), 8 - half, 0)
    return wide[0:1]


def grouped(x):
    return x.reshape(x.shape[0] // 8, 8, x.shape[1])


def rounds_of(size):
    rounds, stride = [], 1
    while stride < size:
        radix = 4 if size // stride % 4 == 0 else 2
        rounds.append((stride, radix))
        stride *= radix
    return rounds


def peer(index, stride, radix, step):
    digit = (index // stride) % radix
    return index + stride * ((digit + step) % radix - digit)


def ring_sum(parts):
    if len(parts) == 4:
        return (parts[0] + parts[2]) + (parts[1] + parts[3])
    return parts[0] + parts[1] if len(parts) == 2 else parts[0]


def kernel(
    sp, tp, q_hbm, k_hbm, v_hbm, g_hbm, qgain_hbm, kgain_hbm, table_hbm,
    qg_ref, kg_ref, vg_ref, out_ref,
    v_ref, k_s, kt_s, qs_s, gs_s, kscale_s, qscale_s, nhat_s, dq_s,
    bias_s, acc_s, clip_s, e_s, dw_s, later_e_s, later_dw_s, peak_s, factor_s, delta_s, ds_s, w_s, gq_s, gk_s,
    nq_s, ng_s, cq_s, bq_s, mid_s, own_s, next_s, before_s, after_s,
    bsum_s, bgot_s, gsum_s, ggot_s, gfirst_s,
    qgain_s, kgain_s, raw_s, wide_s, table_s, gains_s,
    rows_send, rows_recv, back_send, back_recv, part_send, part_recv,
    bias_send, bias_recv, gain_send, gain_recv, load_sem, small_sem,
):
    q_ref, k_ref, g_ref = qg_ref, kg_ref, vg_ref
    tokens = v_ref.shape[0]
    blocks = tokens // BLK
    cross = REACH // BLK
    pairs = nq_s.shape[0]
    tiles, own_tiles = {}, 0
    for qb in range(blocks + cross):
        if qb == blocks:
            own_tiles = len(tiles)
        for kb in range(max(qb - cross, 0), min(qb + 1, blocks)):
            tiles[qb, kb] = len(tiles)
    me = lax.axis_index("sp")
    me_tp = lax.axis_index("tp")
    right, left = lax.rem(me + 1, sp), lax.rem(me + sp - 1, sp)
    rounds = rounds_of(sp)
    count = len(rounds)
    peers = [[{"sp": peer(me, stride, radix, k)} for k in range(1, radix)] for stride, radix in rounds]
    combos = [(k, t) for k in range(rounds[0][1]) for t in range(tp) if k or t]
    nearby = [{"sp": peer(me, 1, rounds[0][1], k), "tp": lax.rem(me_tp + t, tp)} for k, t in combos]
    first, last = me == 0, me == sp - 1
    far = lax.rem(me, PLANE) == 0
    near_by = jnp.logical_not(far)
    has_left, has_right = jnp.logical_not(first), jnp.logical_not(last)

    def tile(j):
        return slice(j * BLK, (j + 1) * BLK)

    def wide_tile(j):
        return slice(j * 2 * BLK, (j + 1) * 2 * BLK)

    def held_at(p, place):
        if place < own_tiles:
            return e_s, dw_s, lax.rem(p, SLOTS), place
        return later_e_s, later_dw_s, lax.rem(p, SLOTS - 1), place - own_tiles

    def lanes_of(p):
        return pl.ds(pl.multiple_of(p * BLK, BLK), BLK)

    def loads(p):
        moves = ((k_hbm, k_ref), (q_hbm, q_ref), (v_hbm, v_ref), (g_hbm, g_ref))
        return [
            pltpu.make_async_copy(src.at[:, lanes_of(p)], dst.at[:, lanes_of(p)], load_sem.at[n, p])
            for n, (src, dst) in enumerate(moves)
        ]

    smalls = [
        pltpu.make_async_copy(src, dst, small_sem.at[n])
        for n, (src, dst) in enumerate(((qgain_hbm, qgain_s), (kgain_hbm, kgain_s), (table_hbm, raw_s)))
    ]
    for copy in smalls:
        copy.start()
    for p in range(pairs):
        for copy in loads(p):
            copy.start()

    barrier = pltpu.get_barrier_semaphore()
    greeted = [{"sp": right}, {"sp": left}] + nearby + [device for group in peers for device in group]
    for device in greeted:
        pl.semaphore_signal(barrier, inc=1, device_id=device, device_id_type=pl.DeviceIdType.MESH)
    def next_bias(p):
        for head in range(2):
            build_bias(table_s[pl.ds(p * 2 + head, 1), :], bias_s.at[lax.rem(p, BIASES)], head)

    pl.semaphore_wait(barrier, len(greeted))

    def remote(src, dst, send, recv, device):
        return pltpu.make_async_remote_copy(
            src_ref=src, dst_ref=dst, send_sem=send, recv_sem=recv,
            device_id=device, device_id_type=pl.DeviceIdType.MESH,
        )

    def row_copies(p):
        rows = slice(0, REACH)
        return (
            remote(q_hbm.at[rows, lanes_of(p)], nq_s.at[p], rows_send.at[0, p], rows_recv.at[0, p], {"sp": left}),
            remote(g_hbm.at[rows, lanes_of(p)], ng_s.at[p], rows_send.at[1, p], rows_recv.at[1, p], {"sp": left}),
        )

    def back_copy(p):
        return remote(cq_s.at[p], bq_s.at[p], back_send.at[p], back_recv.at[p], {"sp": right})

    def own_copy(p):
        return remote(own_s.at[p], after_s.at[p], part_send.at[0, p], part_recv.at[0, p], {"sp": left})

    def next_copy(p):
        return remote(next_s.at[p], before_s.at[p], part_send.at[1, p], part_recv.at[1, p], {"sp": right})

    @pl.when(has_left)
    def _():
        for copy in row_copies(0):
            copy.start()

    @pl.when(has_left)
    def _():
        for copy in row_copies(1):
            copy.start()

    @pl.when(first)
    def _():
        bq_s[...] = jnp.zeros_like(bq_s)
        before_s[...] = jnp.zeros_like(before_s)
        for p in range(pairs):
            before_s[p, 0:cross, :] = jnp.full((cross, 2 * BLK), NEG, F32)

    @pl.when(last)
    def _():
        nq_s[...] = jnp.zeros_like(nq_s)
        ng_s[...] = jnp.zeros_like(ng_s)
        after_s[...] = jnp.zeros_like(after_s)
        for p in range(pairs):
            after_s[p, 0:cross, :] = jnp.full((cross, 2 * BLK), -NEG, F32)
            after_s[p, cross : 2 * cross, :] = jnp.ones((cross, 2 * BLK), F32)

    early = pairs - 1

    def bias_copies(p):
        return [
            remote(bsum_s.at[0, p], bgot_s.at[0, k, p], bias_send.at[0, k, p], bias_recv.at[0, k, p], device)
            for k, device in enumerate(peers[0])
        ]

    def late_copies(r):
        return [
            remote(bsum_s.at[r], bgot_s.at[r, k], bias_send.at[r, k, 0], bias_recv.at[r, k, 0], device)
            for k, device in enumerate(peers[r])
        ]

    def bias_add(r):
        for copy in [copy for p in range(early) for copy in bias_copies(p)] if r == 0 else late_copies(r):
            copy.wait_recv()
        bsum_s[r + 1] = ring_sum([bsum_s[r]] + [bgot_s[r, k] for k in range(len(peers[r]))])
        if r + 1 < count:
            for copy in late_copies(r + 1):
                copy.start()

    def gain_copies(r):
        if r == 0:
            return [
                remote(gsum_s.at[0], gfirst_s.at[n], gain_send.at[0, n], gain_recv.at[0, n], device)
                for n, device in enumerate(nearby)
            ]
        return [
            remote(gsum_s.at[r], ggot_s.at[r, k], gain_send.at[r, k], gain_recv.at[r, k], device)
            for k, device in enumerate(peers[r])
        ]

    def gain_start(r):
        for copy in gain_copies(r):
            copy.start()

    def gain_add(r):
        for copy in gain_copies(r):
            copy.wait_recv()
        if r == 0:
            parts = {combo: gfirst_s[n] for n, combo in enumerate(combos)}
            parts[0, 0] = gsum_s[0]
            gsum_s[1, 0] = ring_sum([parts[k, 0][0] for k in range(rounds[0][1])])
            gsum_s[1, 1] = ring_sum([ring_sum([parts[k, t][1] for t in range(tp)]) for k in range(rounds[0][1])])
        else:
            gsum_s[r + 1] = ring_sum([gsum_s[r]] + [ggot_s[r, k] for k in range(len(peers[r]))])

    gq_s[...] = jnp.zeros_like(gq_s)
    gk_s[...] = jnp.zeros_like(gk_s)

    def query_tile(slot, qb, raw, grad):
        hat, scale = normed(raw, ones)
        qs_s[slot, wide_tile(qb), :] = stack_halves((hat * gain_q).astype(BF16) * jnp.asarray(0.125, BF16))
        gs_s[slot, wide_tile(qb), :] = stack_halves(grad)
        return hat, scale

    def scores(p, slot, qb):
        peaks, sums, deltas = [], [], []
        for kb in range(max(qb - cross, 0), min(qb + 1, blocks)):
            place = tiles[qb, kb]
            j = kb - qb + cross
            s = dot(k_s[slot, tile(kb), :], qs_s[slot, wide_tile(qb), :], ((1,), (1,))) + bias_s[lax.rem(p, BIASES), tile(j), :]
            s = grouped(s)
            peak = jnp.max(s, axis=0)
            e = jnp.exp(s - peak[None])
            dw = dot(v_ref[tile(kb), lanes_of(p)], gs_s[slot, wide_tile(qb), :], ((1,), (1,)))
            e_ref, dw_ref, at, spot = held_at(p, place)
            e_ref[at, spot] = e.reshape(BLK, 2 * BLK)
            dw_ref[at, spot] = dw
            peak_s[slot, place] = peak
            peaks.append(peak)
            sums.append(jnp.sum(e, axis=0))
            deltas.append(jnp.sum(e * grouped(dw), axis=0))
        peak = jnp.max(functools.reduce(jnp.maximum, peaks), axis=0, keepdims=True)
        total = jnp.zeros((8, 2 * BLK), F32)
        delta = jnp.zeros((8, 2 * BLK), F32)
        for part, a, b in zip(peaks, sums, deltas):
            factor = jnp.exp(part - peak)
            total = total + a * factor
            delta = delta + b * factor
        found = (peak, jnp.sum(total, axis=0, keepdims=True), jnp.sum(delta, axis=0, keepdims=True))
        for n, row in enumerate(found):
            if qb < cross:
                own_s[p, n * cross + qb : n * cross + qb + 1, :] = row
            elif qb < blocks:
                mid_s[slot, n : n + 1, :] = row
            else:
                at = n * cross + qb - blocks
                next_s[p, at : at + 1, :] = row

    def inner(p):
        slot = lax.rem(p, SLOTS)
        for copy in loads(p):
            copy.wait()

        def prepare(b):
            hat, scale = normed(k_ref[tile(b), lanes_of(p)], ones)
            kscale_s[slot, tile(b), :] = scale
            unit = hat * gain_k
            k_s[slot, tile(b), :] = unit.astype(BF16)
            kt_s[lax.rem(p, SLOTS + 1), :, tile(b)] = unit.T.astype(BF16)
            _, scale = query_tile(slot, b, q_ref[tile(b), lanes_of(p)], g_ref[tile(b), lanes_of(p)])
            qscale_s[p, tile(b), :] = scale

        for b in range(EARLY):
            prepare(b)
        for b in range(blocks):
            if b + EARLY < blocks:
                prepare(b + EARLY)
            scores(p, slot, b)

        @pl.when(has_left)
        def _():
            own_copy(p).start()

        @pl.when(has_left & near_by & (p == 0))
        def _():
            for copy in row_copies(2):
                copy.start()

    def outer(p):
        slot = lax.rem(p, SLOTS)

        @pl.when(has_right)
        def _():
            for copy in row_copies(p):
                copy.wait_recv()

        for b in range(cross):
            hat, _ = query_tile(slot, blocks + b, nq_s[p, tile(b), :], ng_s[p, tile(b), :])
            nhat_s[slot, tile(b), :] = hat
        past = jnp.maximum(p - 3, 0)
        for b in range(cross):
            rest_query(past, b, p >= 3)
            scores(p, slot, blocks + b)
        for b in range(cross, blocks):
            rest_query(past, b, p >= 3)
        bsum_s[0, past] = rest_bias(past)
        next_bias(jnp.minimum(p + 2, pairs - 1))

        @pl.when(has_right)
        def _():
            next_copy(p).start()

    def settle(mine, other):
        here, there = mine[:cross], other[:cross]
        peak = jnp.maximum(here, there)
        a, b = jnp.exp(here - peak), jnp.exp(there - peak)
        total = mine[cross : 2 * cross] * a + other[cross : 2 * cross] * b
        delta = mine[2 * cross : 3 * cross] * a + other[2 * cross : 3 * cross] * b
        inverse = 1.0 / total
        return peak, inverse, delta * inverse

    def backward(p):
        slot = lax.rem(p, SLOTS)

        @pl.when(has_left)
        def _():
            next_copy(p).wait_recv()

        @pl.when(has_right)
        def _():
            own_copy(p).wait_recv()

        @pl.when(has_left & (p + 3 < pairs) & (p <= 1) & far)
        def _():
            for copy in row_copies(p + 3):
                copy.start()

        own = settle(own_s[p], before_s[p])
        later = settle(next_s[p], after_s[p])
        inverse = 1.0 / mid_s[slot, 1:2, :]
        mid = (mid_s[slot, 0:1, :], inverse, mid_s[slot, 2:3, :] * inverse)
        for qb in range(blocks + cross):
            found, at = (own, qb) if qb < cross else (mid, 0) if qb < blocks else (later, qb - blocks)
            peak, inverse, delta = (x[at : at + 1] for x in found)
            delta_s[qb] = jnp.broadcast_to(delta, (8, 2 * BLK))
            for kb in range(max(qb - cross, 0), min(qb + 1, blocks)):
                place = tiles[qb, kb]
                factor_s[place] = jnp.exp(peak_s[slot, place] - peak) * inverse

        clipped = jnp.zeros((8, 2 * BLK), F32)
        gain_sum = jnp.zeros((1, BLK), F32)
        for kb in reversed(range(blocks)):
            for qb in range(kb, kb + cross + 1):
                place, j = tiles[qb, kb], kb - qb + cross
                e_ref, dw_ref, held, spot = held_at(p, place)
                for part in range(BLK // PART):
                    rows = slice(part * PART, (part + 1) * PART)
                    w = grouped(e_ref[held, spot, rows, :]) * factor_s[place][None]
                    ds = w * (grouped(dw_ref[held, spot, rows, :]) - delta_s[qb][None])
                    if j < 2:
                        clipped = clipped + jnp.sum(ds, axis=0)
                    ds, w = ds.reshape(PART, 2 * BLK), w.reshape(PART, 2 * BLK)
                    if j >= 2:
                        at = slice((j - 2) * BLK + part * PART, (j - 2) * BLK + (part + 1) * PART)
                        acc_s[at, :] = ds if kb == blocks - 1 else acc_s[at, :] + ds
                    at = slice(kb * BLK + part * PART, kb * BLK + (part + 1) * PART)
                    ds_s[at, wide_tile(qb)] = ds.astype(BF16)
                    w_s[at, wide_tile(qb)] = w.astype(BF16)
            near = slice(kb * 2 * BLK, blocks * 2 * BLK)
            away = slice(blocks * 2 * BLK, (kb + cross + 1) * 2 * BLK)
            dk = dot(ds_s[tile(kb), near], qs_s[slot, near, :], ((1,), (0,)))
            dv = dot(w_s[tile(kb), near], gs_s[slot, near, :], ((1,), (0,)))
            if kb + cross >= blocks:
                dk = dk + dot(ds_s[tile(kb), away], qs_s[slot, away, :], ((1,), (0,))).astype(BF16).astype(F32)
                dv = dv + dot(w_s[tile(kb), away], gs_s[slot, away, :], ((1,), (0,))).astype(BF16).astype(F32)
            hat = k_ref[tile(kb), lanes_of(p)].astype(F32) * kscale_s[slot, tile(kb), :]
            gain_sum = gain_sum + jnp.sum(dk * hat, axis=0, keepdims=True)
            kg_ref[tile(kb), lanes_of(p)] = norm_grad(dk, gain_k, hat, kscale_s[slot, tile(kb), :], ones).astype(BF16)
            vg_ref[tile(kb), lanes_of(p)] = dv.astype(BF16)
            if kb > 0:
                query_side(p, slot, kb + cross)
        gk_s[...] += gain_sum
        clip_s[...] = clipped

        @pl.when(has_right)
        def _():
            back_copy(p).start()

    def turned(p, qb):
        keys = slice(max(qb - cross, 0) * BLK, min(qb + 1, blocks) * BLK)
        dqt = dot(kt_s[lax.rem(p, SLOTS + 1), :, keys], ds_s[keys, wide_tile(qb)], ((1,), (0,)))
        dqt = jnp.concatenate([dqt[:64, :BLK], dqt[64:, BLK:]], axis=0)
        return dqt.T * 0.125

    def query_side(p, slot, qb):
        dq = turned(p, qb)
        cq_s[p, tile(qb - blocks), :] = dq.astype(BF16)
        gq_s[...] += jnp.sum(dq * nhat_s[slot, tile(qb - blocks), :], axis=0, keepdims=True)

    def rest_query(p, qb, live):
        dq = turned(p, qb)
        dq_s[p, tile(qb), :] = dq
        hat = q_ref[tile(qb), lanes_of(p)].astype(F32) * qscale_s[p, tile(qb), :]
        part = jnp.sum(dq * hat, axis=0, keepdims=True)
        gq_s[...] += jnp.where(live, part, 0.0)

    def rest_bias(p):
        lane = lax.broadcasted_iota(jnp.int32, (1, 512), 1)
        rows = []
        clipped = jnp.sum(clip_s[...], axis=0, keepdims=True)
        for head in range(2):
            far = jnp.sum(clipped[:, head * BLK : (head + 1) * BLK], axis=1, keepdims=True)
            row = fold_bias(acc_s, head) + jnp.where(lane == 0, far, 0.0)
            rows += [row[:, b * BLK : (b + 1) * BLK] for b in range(4)]
        return jnp.concatenate(rows, axis=0)

    def finish(p, _):
        @pl.when(has_left)
        def _():
            back_copy(p).wait_recv()

        for b in range(blocks):
            dq = dq_s[p, tile(b), :]
            if b < cross:
                dq = dq + bq_s[p, tile(b), :].astype(F32)
            scale = qscale_s[p, tile(b), :]
            hat = q_ref[tile(b), lanes_of(p)].astype(F32) * scale
            grad = norm_grad(dq, gain_q, hat, scale, ones)
            qg_ref[tile(b), lanes_of(p)] = grad.astype(BF16)

        @pl.when(has_left)
        def _():
            for copy in (*row_copies(p), own_copy(p)):
                copy.wait_send()

        @pl.when(has_right)
        def _():
            for copy in (back_copy(p), next_copy(p)):
                copy.wait_send()

        return 0

    def step(t, _):
        @pl.when(t < pairs)
        def _():
            inner(t)

        @pl.when(has_left & (t < pairs) & (t == 2) & far)
        def _():
            for copy in row_copies(t):
                copy.start()

        @pl.when((t >= 1) & (t <= pairs))
        def _():
            outer(t - 1)

        @pl.when(has_left & (t + 2 < pairs) & (t >= 1) & near_by)
        def _():
            for copy in row_copies(t + 2):
                copy.start()

        @pl.when(t > pairs)
        def _():
            for qb in range(blocks):
                rest_query(t - 4, qb, True)
            bsum_s[0, t - 4] = rest_bias(t - 4)

        @pl.when(t >= 4)
        def _():
            for copy in bias_copies(t - 4):
                copy.start()

        @pl.when(t >= 3)
        def _():
            backward(t - 3)

        @pl.when(has_left & (t >= 4) & (t + 1 < pairs) & far)
        def _():
            for copy in row_copies(t + 1):
                copy.start()

        return 0

    ones = half_ones()
    for copy in smalls:
        copy.wait()
    for half in range(2):
        gains_s[0:1, half * 64 : half * 64 + 64] = qgain_s[...].astype(F32)
        gains_s[1:2, half * 64 : half * 64 + 64] = kgain_s[...].astype(F32)
    gain_q = gains_s[0:1, :]
    gain_k = gains_s[1:2, :]
    heads, span = raw_s.shape
    wide_s[...] = jnp.zeros_like(wide_s)
    wide_s[0:heads, 0:span] = raw_s[...].astype(F32)
    wide = wide_s[...]
    place = lax.broadcasted_iota(jnp.int32, wide.shape, 1)
    moved = pltpu.roll(wide, 193, 1)
    table_s[...] = jnp.where(place <= 128, wide[:, span - 1 : span], jnp.where(place < 193, NEG, moved))

    for p in range(min(2, pairs)):
        next_bias(p)
    lax.fori_loop(0, pairs + 3, step, 0)
    for qb in range(blocks):
        rest_query(pairs - 1, qb, True)
    gsum_s[0, 0] = rest_bias(pairs - 1)
    gsum_s[0, 1] = jnp.zeros(gsum_s.shape[2:], F32)
    gsum_s[0, 1, 0:1, :] = gq_s[...]
    gsum_s[0, 1, 1:2, :] = gk_s[...]
    gain_start(0)
    for r in range(count):
        bias_add(r)
        if r == 0:
            lax.fori_loop(0, pairs // 2, finish, 0)
        gain_add(r)
        if r + 1 < count:
            gain_start(r + 1)
        if r == 0:
            lax.fori_loop(pairs // 2, pairs, finish, 0)
    for p in range(early):
        out_ref[p] = bsum_s[count, p]
    out_ref[early] = gsum_s[count, 0]
    out_ref[pairs] = gsum_s[count, 1]
    for p in range(early):
        for copy in bias_copies(p):
            copy.wait_send()
    for r in range(count):
        if r > 0:
            for copy in late_copies(r):
                copy.wait_send()
        for copy in gain_copies(r):
            copy.wait_send()


def drain(
    qg_ref, kg_ref, vg_ref, stat_ref, qg_hbm, kg_hbm, vg_hbm, bias_hbm, gq_hbm, gk_hbm,
    wide_s, bias_s, gq_s, gk_s, sem,
):
    moves = [(qg_ref, qg_hbm), (kg_ref, kg_hbm), (vg_ref, vg_hbm), (gq_s, gq_hbm), (gk_s, gk_hbm), (bias_s, bias_hbm)]
    copies = [pltpu.make_async_copy(src, dst, sem.at[n]) for n, (src, dst) in enumerate(moves)]
    for copy in copies[:3]:
        copy.start()
    heads, span = bias_s.shape
    pairs = heads // 2
    for row, ref in enumerate((gq_s, gk_s)):
        both = stat_ref[pairs, row : row + 1, :]
        ref[...] = (both + pltpu.roll(both, 64, 1))[:, :64].reshape(64)
    copies[3].start()
    copies[4].start()
    wide_s[...] = jnp.zeros_like(wide_s)
    for head in range(heads):
        for b in range(4):
            row = head % 2 * 4 + b
            wide_s[head : head + 1, b * BLK : (b + 1) * BLK] = stat_ref[head // 2, row : row + 1, :]
    wide = wide_s[...]
    lane = lax.broadcasted_iota(jnp.int32, wide.shape, 1)
    far = jnp.sum(jnp.where(lane <= 128, wide, 0.0), axis=1, keepdims=True)
    folded = jnp.where(lane == span - 1, far, pltpu.roll(wide, 319, 1))
    bias_s[...] = folded[:heads, :span]
    copies[5].start()
    for copy in copies:
        copy.wait()


def body(query_rows, key_rows, value_rows, query_gain, key_gain, position_bias, output_grad):
    heads = position_bias.shape[0]
    pairs = heads // 2
    tokens = query_rows.shape[0]
    sp, tp = lax.axis_size("sp"), lax.axis_size("tp")
    count = len(rounds_of(sp))
    group = 4 * tp
    ext = tokens + REACH
    reach, blocks = REACH // BLK, tokens // BLK
    held = (reach + 1) * blocks
    own = sum(min(qb, reach) + 1 for qb in range(blocks))
    padded = (heads + 7) // 8 * 8
    vmem, hbm = pl.BlockSpec(memory_space=pltpu.VMEM), pl.BlockSpec(memory_space=pltpu.HBM)
    shape = jax.ShapeDtypeStruct
    grads = shape((tokens, heads * 64), BF16)
    sems = pltpu.SemaphoreType.DMA
    operands = (
        query_rows, key_rows, value_rows, output_grad,
        query_gain.reshape(1, 64), key_gain.reshape(1, 64), position_bias,
    )
    results = pl.pallas_call(
        functools.partial(kernel, sp, tp),
        in_specs=[hbm] * 7,
        out_specs=[vmem] * 4,
        out_shape=[grads, grads, grads, shape((pairs + 1, 8, BLK), F32)],
        scratch_shapes=[pltpu.VMEM((tokens, heads * 64), BF16)]
        + [
            pltpu.VMEM((SLOTS, tokens, BLK), BF16), pltpu.VMEM((SLOTS + 1, BLK, tokens), BF16),
            pltpu.VMEM((SLOTS, ext * 2, BLK), BF16), pltpu.VMEM((SLOTS, ext * 2, BLK), BF16),
            pltpu.VMEM((SLOTS, tokens, BLK), F32), pltpu.VMEM((pairs, tokens, BLK), F32),
            pltpu.VMEM((SLOTS, REACH, BLK), F32), pltpu.VMEM((pairs, tokens, BLK), F32),
            pltpu.VMEM((BIASES, BAND, 2 * BLK), F32), pltpu.VMEM((3 * BLK, 2 * BLK), F32), pltpu.VMEM((8, 2 * BLK), F32),
            *[pltpu.VMEM((SLOTS, own, BLK, 2 * BLK), F32)] * 2, *[pltpu.VMEM((SLOTS - 1, held - own, BLK, 2 * BLK), F32)] * 2,
            pltpu.VMEM((SLOTS, held, 8, 2 * BLK), F32), pltpu.VMEM((held, 8, 2 * BLK), F32),
            pltpu.VMEM((ext // BLK, 8, 2 * BLK), F32),
            pltpu.VMEM((tokens, ext * 2), BF16), pltpu.VMEM((tokens, ext * 2), BF16),
            pltpu.VMEM((1, BLK), F32), pltpu.VMEM((1, BLK), F32),
        ]
        + [pltpu.VMEM((pairs, REACH, BLK), BF16)] * 4
        + [pltpu.VMEM((SLOTS, 8, 2 * BLK), F32)]
        + [pltpu.VMEM((pairs, 16, 2 * BLK), F32)] * 4
        + [
            pltpu.VMEM((count + 1, pairs - 1, 8, BLK), F32), pltpu.VMEM((count, 3, pairs - 1, 8, BLK), F32),
            pltpu.VMEM((count + 1, 2, 8, BLK), F32), pltpu.VMEM((count, 3, 2, 8, BLK), F32), pltpu.VMEM((group, 2, 8, BLK), F32),
            pltpu.VMEM((1, 64), BF16), pltpu.VMEM((1, 64), BF16), pltpu.VMEM(position_bias.shape, BF16),
            pltpu.VMEM((padded, 512), F32), pltpu.VMEM((padded, 512), F32), pltpu.VMEM((8, BLK), F32),
            sems((2, pairs)), sems((2, pairs)), sems((pairs,)), sems((pairs,)), sems((2, pairs)), sems((2, pairs)),
            sems((count, 3, pairs)), sems((count, 3, pairs)), sems((count, group)), sems((count, group)),
            sems((4, pairs)), sems((3,)),
        ],
        compiler_params=pltpu.CompilerParams(collective_id=0, has_side_effects=True, vmem_limit_bytes=50 << 20),
        name="attend",
    )(*[pltpu.with_memory_space_constraint(x, pltpu.HBM) for x in operands])
    return pl.pallas_call(
        drain,
        in_specs=[vmem] * 4,
        out_specs=[hbm] * 6,
        out_shape=[grads, grads, grads, shape(position_bias.shape, F32), shape((64,), F32), shape((64,), F32)],
        scratch_shapes=[
            pltpu.VMEM((padded, 512), F32), pltpu.VMEM(position_bias.shape, F32),
            pltpu.VMEM((64,), F32), pltpu.VMEM((64,), F32), sems((6,)),
        ],
        compiler_params=pltpu.CompilerParams(vmem_limit_bytes=2 << 20),
        name="drain",
    )(*results)


def solution(mesh):
    placed = (P("sp", "tp"), P("sp", "tp"), P("sp", "tp"), P(), P(), P("tp", None), P("sp", "tp"))
    return jax.shard_map(
        body,
        mesh=mesh,
        in_specs=placed,
        out_specs=(P("sp", "tp"), P("sp", "tp"), P("sp", "tp"), P("tp", None), P(), P()),
        check_vma=False,
    )
```
